32 devices in a mesh: grp: 2 (over y), ep: 4 (over z), tp: 4 (over x, core).
Axes of the slice: x: 2, y: 2, z: 4, core: 2. Of those that a mesh axis runs over, the one named last changes fastest.
Arguments:
- mix_query: bfloat16 [4096, 16, 128], P(('grp', 'ep'), 'tp'), parts along dimension 0, may hold values from -6 to 6
- mix_keys: bfloat16 [4096, 16, 128], P(('grp', 'ep'), 'tp'), parts along dimension 0, may hold values from -6 to 6
- mix_values: bfloat16 [4096, 16, 128], P(('grp', 'ep'), 'tp'), parts along dimension 0, may hold values from -6 to 6
- beta_in: float32 [16, 4096], P('tp', ('grp', 'ep')), parts along dimension 1, may hold values from -9.5 to 6
- decay_in: float32 [16, 4096], P('tp', ('grp', 'ep')), parts along dimension 1, may hold values from -14 to 0
- norm_gain: float32 [128], replicated, may hold values from 0.1 to 1.9
- ffn_input: bfloat16 [1024, 4096], P(('grp', 'ep'), 'tp'), parts along dimension 0, may hold values from -200 to 200
- ffn_gain: float32 [4096], P('tp'), may hold values from 0.1 to 1.9
- expert_ids: int32 [1024, 2], P(('grp', 'ep')), parts along dimension 0, may hold values from 0 to 15, as said below
- expert_share: float32 [1024, 2], P(('grp', 'ep')), parts along dimension 0, may hold values from 0.2 to 1
- w_gate: bfloat16 [16, 4096, 1024], P('ep', None, 'tp'), may hold values from -0.09375 to 0.09375
- w_up: bfloat16 [16, 4096, 1024], P('ep', None, 'tp'), may hold values from -0.09375 to 0.09375
- w_down: bfloat16 [16, 1024, 4096], P('ep', None, 'tp'), may hold values from -0.1875 to 0.1875
Outputs:
- mix_out: bfloat16 [4096, 16, 128], P(('grp', 'ep'), 'tp'), parts along dimension 0
- ffn_out: bfloat16 [1024, 4096], P(('grp', 'ep'), 'tp'), parts along dimension 0
The draws below stay inside these ranges and needn't reach their ends.
There are 2 independent parts, one for each index of `grp`. The reference program is written for one: setup_inputs(seed, part) draws one part's arguments, and reference() takes and returns one part's arrays. A program takes and returns all parts, laid end to end along the dimension named above; an argument that names none is the same for every part. Nothing has to cross between parts.
Inputs may be any that keep to these rules, and one draw needn't show every extreme that they name: `expert_ids`: each row names two different experts of one group, the group being id // 4; the rows of one device (aligned blocks of 128 rows) name every expert exactly 2 * 128 // 16 times.
All inputs are finite; a program needn't handle non-finite values.
Results may differ from the reference program's by a relative error of at most 0.007.
Values may be sent and summed in bfloat16 or wider, within the bound.
A program may use at most 128 MiB of HBM per device.

```python
import math
import jax
import jax.numpy as jnp
from jax import lax

D = 4096
HEADS = 16
HD = 128
BLOCK = 64
SEQ_DEV = 512
SEQUENCE_LENGTH = 2048
FF = 1024
GROUPS = 4
GROUP_SIZE = 4
EXPERTS = 16
RB_EP = 128
TB = 512


def draw_beta_in(key, part):
    token_sequence = jax.random.split(jax.random.fold_in(key, 11), 2)
    weak_heads = (jax.random.permutation(token_sequence[0], HEADS) < HEADS // 2)[:, None]
    centre = jnp.where(weak_heads, -5.3, 0.0)
    spread = jnp.where(weak_heads, 1.0, 1.5)
    noise = jax.random.truncated_normal(token_sequence[1], -4.0, 4.0, (HEADS, SEQUENCE_LENGTH), jnp.float32)
    return centre + spread * noise


def draw_decay_in(key, part):
    token_sequence = jax.random.split(key, 4)
    head_log_decay = jax.random.uniform(token_sequence[0], (HEADS, 1), jnp.float32, math.log(3e-05), math.log(0.03))
    span_count = 2 * (SEQUENCE_LENGTH // SEQ_DEV)
    span_index = jnp.arange(SEQUENCE_LENGTH) * span_count // SEQUENCE_LENGTH
    span_table = jnp.exp(jax.random.uniform(token_sequence[1], (HEADS, span_count), jnp.float32, math.log(0.5), math.log(2.0)))
    position_values = span_table[:, span_index]
    random_offset = jnp.exp(jax.random.uniform(token_sequence[2], (HEADS, SEQUENCE_LENGTH), jnp.float32, -0.5, 0.5))
    spike_position = jax.random.randint(token_sequence[3], (6,), 0, SEQUENCE_LENGTH)
    spike_tokens = jnp.any(jnp.arange(SEQUENCE_LENGTH)[None, :] == spike_position[:, None], axis=0).astype(jnp.float32)
    decay_rate_rows = jnp.exp(head_log_decay) * position_values * random_offset + 0.4 * spike_tokens[None, :]
    return jnp.log(jnp.expm1(decay_rate_rows))


def draw_ffn_input(key, part):
    token_sequence = jax.random.split(key, 3)
    columns = jnp.arange(D, dtype=jnp.float32) / D
    column_scale = jnp.exp(math.log(3.0) * columns + jax.random.uniform(token_sequence[0], (D,), jnp.float32, -0.4, 0.4))
    base_values = jax.random.truncated_normal(token_sequence[1], -4.0, 4.0, (TB, D), jnp.float32)
    row_scale = jnp.exp(jax.random.uniform(token_sequence[2], (TB, 1), jnp.float32, 0.0, math.log(10.0)))
    return (base_values * row_scale * column_scale[None, :]).astype(jnp.bfloat16)


def draw_expert_ids(key, part):
    source_count = TB // RB_EP
    block_keys = jax.random.split(key, source_count)
    rank_values = jax.vmap(lambda one_key: jax.random.permutation(one_key, RB_EP))(block_keys).reshape(-1)
    group_of = rank_values % GROUPS
    within = rank_values // GROUPS
    first_pick = within % GROUP_SIZE
    second = (first_pick + 1 + within // GROUP_SIZE % (GROUP_SIZE - 1)) % GROUP_SIZE
    return jnp.stack([group_of * GROUP_SIZE + first_pick, group_of * GROUP_SIZE + second], axis=1).astype(jnp.int32)


def block_levels(own_key, shape, pieces, smallest, largest):
    def one(dim, blocks):
        draws = jax.random.uniform(jax.random.fold_in(jax.random.fold_in(own_key, 6), dim), (blocks,), jnp.float32, smallest / len(pieces), largest / len(pieces))
        return jnp.repeat(jnp.exp(draws), shape[dim] // blocks).reshape((-1,) + (1,) * (len(shape) - dim - 1))

    loudness = one(*pieces[0])
    for cut in pieces[1:]:
        loudness = loudness * one(*cut)
    return loudness


def centred(stream_key, shape, scale, bound, cuts=(), held_as=jnp.bfloat16):
    factor_of = block_levels(stream_key, shape, cuts, -0.22, 0.18) if cuts else 1.0
    drawn = jax.random.normal(stream_key, shape, jnp.float32) * scale * factor_of
    return jnp.minimum(jnp.maximum(drawn, -bound), bound).astype(held_as)


def setup_inputs(seed: int = 0, part: int = 0) -> dict:
    streams_of = jax.random.split(jax.random.key(seed), 14)
    part_keys = jax.random.split(jax.random.fold_in(streams_of[13], part), 14)
    return {
        "mix_query": centred(part_keys[0], (SEQUENCE_LENGTH, HEADS, HD), 1.0, 6.0, ((0, 4), (1, 4))),
        "mix_keys": centred(part_keys[1], (SEQUENCE_LENGTH, HEADS, HD), 1.0, 6.0, ((0, 4), (1, 4))),
        "mix_values": centred(part_keys[2], (SEQUENCE_LENGTH, HEADS, HD), 1.0, 6.0, ((0, 4), (1, 4))),
        "beta_in": draw_beta_in(jax.random.fold_in(jax.random.fold_in(streams_of[13], part), 71), part),
        "decay_in": draw_decay_in(jax.random.fold_in(jax.random.fold_in(streams_of[13], part), 71), part),
        "norm_gain": jnp.clip(1.0 + 0.18 * jax.random.normal(streams_of[5], (HD,), jnp.float32), 0.1, 1.9),
        "ffn_input": draw_ffn_input(jax.random.fold_in(jax.random.fold_in(streams_of[13], part), 71), part),
        "ffn_gain": jnp.clip(1.0 + 0.18 * jax.random.normal(streams_of[7], (D,), jnp.float32), 0.1, 1.9),
        "expert_ids": draw_expert_ids(jax.random.fold_in(jax.random.fold_in(streams_of[13], part), 71), part),
        "expert_share": jnp.clip(0.2 + 0.8 * jax.random.uniform(part_keys[9], (TB, 2), jnp.float32) ** block_levels(part_keys[9], (TB, 2), ((0, 4),), -0.2, 0.2), 0.2, 1.0),
        "w_gate": centred(streams_of[10], (EXPERTS, D, FF), D ** -0.5, 0.09375, ((0, 4), (2, 4))),
        "w_up": centred(streams_of[11], (EXPERTS, D, FF), D ** -0.5, 0.09375, ((0, 4), (2, 4))),
        "w_down": centred(streams_of[12], (EXPERTS, FF, D), FF ** -0.5, 0.1875, ((0, 4), (2, 4))),
    }


PRECISE = lax.Precision.HIGHEST
EPSILON = 1e-06

def unit_inverse(strict_lower):
    extent = strict_lower.shape[-1]
    identity = jnp.eye(extent, dtype=jnp.float32)
    powered = -strict_lower
    product = identity + powered
    for section_index in range(1, (extent - 1).bit_length()):
        powered = jnp.matmul(powered, powered, precision=PRECISE)
        product = jnp.matmul(product, identity + powered, precision=PRECISE)
    return product

def block_terms(queries, keyset, valueset, betas, rates):
    extent = queries.shape[-2]
    cumulative = -jnp.cumsum(rates, axis=-1)
    positions = jnp.arange(extent)
    causal = positions[:, None] >= positions[None, :]
    strict = positions[:, None] > positions[None, :]
    spread = cumulative[..., :, None] - cumulative[..., None, :]
    decay_mask = jnp.where(causal, jnp.exp(jnp.where(causal, spread, 0.0)), 0.0)
    keys_beta = keyset * betas[..., None]
    values_beta = valueset * betas[..., None]
    lower_part = jnp.where(strict, jnp.einsum('...id,...jd->...ij', keys_beta, keyset, precision=PRECISE) * decay_mask, 0.0)
    inverse = unit_inverse(lower_part)
    update = jnp.einsum('...ij,...jd->...id', inverse, values_beta, precision=PRECISE)
    correction = jnp.einsum('...ij,...jd->...id', inverse, keys_beta * jnp.exp(cumulative)[..., None], precision=PRECISE)
    scores = jnp.where(causal, jnp.einsum('...id,...jd->...ij', queries, keyset, precision=PRECISE) * decay_mask, 0.0)
    query_decay = queries * jnp.exp(cumulative)[..., None]
    key_decay = keyset * jnp.exp(cumulative[..., -1:] - cumulative)[..., None]
    block_decay = jnp.exp(cumulative[..., -1])
    return (query_decay, key_decay, update, correction, scores, block_decay)

def unit_rows(values_in, factor):
    floats = values_in.astype(jnp.float32)
    return floats * lax.rsqrt(lax.optimization_barrier(jnp.sum(floats * floats, -1, keepdims=True)) + EPSILON) * factor

def mixer_reference(mix_query, mix_keys, mix_values, beta_in, decay_in, norm_gain):
    length, head_count, width = mix_query.shape
    blocks = length // BLOCK

    def to_blocks(tensor):
        return tensor.reshape(blocks, BLOCK, head_count, width).transpose(0, 2, 1, 3)
    queries = to_blocks(unit_rows(mix_query, width ** (-0.5)))
    keyset = to_blocks(unit_rows(mix_keys, 1.0))
    valueset = to_blocks(mix_values.astype(jnp.float32))
    betas = jax.nn.sigmoid(beta_in).reshape(head_count, blocks, BLOCK).transpose(1, 0, 2)
    rates = jax.nn.softplus(decay_in).reshape(head_count, blocks, BLOCK).transpose(1, 0, 2)

    def advance(carried, inputs):
        query_decay, key_decay, update, correction, scores, block_decay = block_terms(*inputs)
        fresh = update - jnp.einsum('hcd,hde->hce', correction, carried, precision=PRECISE)
        output = jnp.einsum('hcd,hde->hce', query_decay, carried, precision=PRECISE) + jnp.einsum('hij,hje->hie', scores, fresh, precision=PRECISE)
        carried = carried * block_decay[:, None, None] + jnp.einsum('hcd,hce->hde', key_decay, fresh, precision=PRECISE)
        return (carried, output)
    initial = jnp.zeros((head_count, width, width), jnp.float32)
    ignored, outputs = lax.scan(advance, initial, (queries, keyset, valueset, betas, rates))
    raw_mix = outputs.transpose(0, 2, 1, 3).reshape(length, head_count, width)
    return (raw_mix * lax.rsqrt(lax.optimization_barrier(jnp.mean(raw_mix * raw_mix, -1, keepdims=True)) + EPSILON) * norm_gain).astype(jnp.bfloat16)

def experts_reference(ffn_input, ffn_gain, expert_ids, expert_share, w_gate, w_up, w_down):
    floats = ffn_input.astype(jnp.float32)
    normed = (floats * lax.rsqrt(lax.optimization_barrier(jnp.mean(floats * floats, -1, keepdims=True)) + EPSILON) * ffn_gain).astype(jnp.bfloat16)
    pick_count = expert_ids.shape[1]
    flat_ids = expert_ids.reshape(-1)
    sort_order = jnp.argsort(flat_ids, stable=True).astype(jnp.int32)
    source_rows = (sort_order // pick_count).reshape(w_gate.shape[0], -1)

    def one_expert(inputs):
        rows_here, gate_weight, up_weight, down_weight = inputs
        chosen = normed[rows_here]
        gate_sum = jnp.dot(chosen, gate_weight, preferred_element_type=jnp.float32)
        up_sum = jnp.dot(chosen, up_weight, preferred_element_type=jnp.float32)
        hidden = (jax.nn.silu(gate_sum) * up_sum).astype(jnp.bfloat16)
        return jnp.dot(hidden, down_weight, preferred_element_type=jnp.float32).astype(jnp.bfloat16)
    copies = lax.map(one_expert, (source_rows, w_gate, w_up, w_down)).reshape(-1, normed.shape[1])
    slots = jnp.argsort(sort_order).astype(jnp.int32)
    per_slot = copies[slots].reshape(expert_ids.shape[0], pick_count, -1)
    return lax.optimization_barrier(jnp.sum(per_slot.astype(jnp.float32) * expert_share[..., None], axis=1)).astype(jnp.bfloat16)

def reference(mix_query, mix_keys, mix_values, beta_in, decay_in, norm_gain, ffn_input, ffn_gain, expert_ids, expert_share, w_gate, w_up, w_down):
    mix_out = mixer_reference(mix_query, mix_keys, mix_values, beta_in, decay_in, norm_gain)
    ffn_out = experts_reference(ffn_input, ffn_gain, expert_ids, expert_share, w_gate, w_up, w_down)
    return (mix_out, ffn_out)
```

```python
import functools
import jax
import jax.numpy as jnp
from jax import lax
from jax.experimental import pallas as pl
from jax.experimental.pallas import tpu as pltpu
from jax.sharding import PartitionSpec as P

BLOCK = 64
GROUP = 4
F32 = jnp.float32
BF16 = jnp.bfloat16
MESH = pl.DeviceIdType.MESH
ROWS_COLS = (((1,), (0,)), ((), ()))
ROWS_ROWS = (((1,), (1,)), ((), ()))
COLS_COLS = (((0,), (0,)), ((), ()))


PRECISE = lax.Precision.HIGHEST
EPSILON = 1e-06


def entering_2(value, axis, join, neutral):
    count, mine = (lax.axis_size(axis), lax.axis_index(axis))
    pieces = jax.tree.map(lambda part: lax.all_gather(part, axis), value)
    subtotal = jax.tree.map(
        lambda part, zero: jnp.full_like(part, 0) + jnp.asarray(zero, part.dtype), value, neutral
    )

    def turn(position, subtotal):
        longer = join(subtotal, jax.tree.map(lambda part: part[position], pieces))
        return jax.tree.map(lambda new, old: jnp.where(position < mine, new, old), longer, subtotal)

    return lax.fori_loop(0, count - 1, turn, subtotal)


def unit_inverse(strict_lower):
    extent = strict_lower.shape[-1]
    identity = jnp.eye(extent, dtype=jnp.float32)
    powered = -strict_lower
    product = identity + powered
    for section_index in range(1, (extent - 1).bit_length()):
        powered = jnp.matmul(powered, powered, precision=PRECISE)
        product = jnp.matmul(product, identity + powered, precision=PRECISE)
    return product


def block_terms(queries, keyset, valueset, betas, rates):
    extent = queries.shape[-2]
    cumulative = -jnp.cumsum(rates, axis=-1)
    positions = jnp.arange(extent)
    causal = positions[:, None] >= positions[None, :]
    strict = positions[:, None] > positions[None, :]
    spread = cumulative[..., :, None] - cumulative[..., None, :]
    decay_mask = jnp.where(causal, jnp.exp(jnp.where(causal, spread, 0.0)), 0.0)
    keys_beta = keyset * betas[..., None]
    values_beta = valueset * betas[..., None]
    lower_part = jnp.where(
        strict,
        jnp.einsum("...id,...jd->...ij", keys_beta, keyset, precision=PRECISE) * decay_mask,
        0.0,
    )
    inverse = unit_inverse(lower_part)
    update = jnp.einsum("...ij,...jd->...id", inverse, values_beta, precision=PRECISE)
    correction = jnp.einsum(
        "...ij,...jd->...id", inverse, keys_beta * jnp.exp(cumulative)[..., None], precision=PRECISE
    )
    scores = jnp.where(
        causal,
        jnp.einsum("...id,...jd->...ij", queries, keyset, precision=PRECISE) * decay_mask,
        0.0,
    )
    query_decay = queries * jnp.exp(cumulative)[..., None]
    key_decay = keyset * jnp.exp(cumulative[..., -1:] - cumulative)[..., None]
    block_decay = jnp.exp(cumulative[..., -1])
    return (query_decay, key_decay, update, correction, scores, block_decay)


def unit_rows(values_in, factor):
    floats = values_in.astype(jnp.float32)
    return floats * lax.rsqrt(jnp.sum(floats * floats, -1, keepdims=True) + EPSILON) * factor


def compose(earlier, later):
    return (
        jnp.matmul(later[0], earlier[0], precision=PRECISE),
        jnp.matmul(later[0], earlier[1], precision=PRECISE) + later[1],
    )


def mixer_body(mix_query, mix_keys, mix_values, beta_in, decay_in, norm_gain):
    length, head_count, width = mix_query.shape
    blocks = length // BLOCK

    def to_blocks(tensor):
        return tensor.reshape(blocks, BLOCK, head_count, width).transpose(2, 0, 1, 3)

    queries = to_blocks(unit_rows(mix_query, width ** (-0.5)))
    keyset = to_blocks(unit_rows(mix_keys, 1.0))
    valueset = to_blocks(mix_values.astype(jnp.float32))
    betas = jax.nn.sigmoid(beta_in).reshape(head_count, blocks, BLOCK)
    rates = jax.nn.softplus(decay_in).reshape(head_count, blocks, BLOCK)
    query_decay, key_decay, update, correction, scores, block_decay = block_terms(
        queries, keyset, valueset, betas, rates
    )
    identity = jnp.eye(width, dtype=jnp.float32)
    transfer = block_decay[..., None, None] * identity - jnp.einsum(
        "hncd,hnce->hnde", key_decay, correction, precision=PRECISE
    )
    offset = jnp.einsum("hncd,hnce->hnde", key_decay, update, precision=PRECISE)
    prefix_map, prefix_add = lax.associative_scan(compose, (transfer, offset), axis=1)
    total_map = prefix_map[:, -1]
    total_add = prefix_add[:, -1]
    empty_state = jnp.zeros((head_count, width, width), jnp.float32)
    unit_maps = jnp.broadcast_to(identity, (head_count, width, width))
    ignored_map, entering = entering_2(
        (total_map, total_add), "ep", compose, (unit_maps, empty_state)
    )
    after_blocks = jnp.matmul(prefix_map, entering[:, None], precision=PRECISE) + prefix_add
    starts = jnp.concatenate([entering[:, None], after_blocks[:, :-1]], axis=1)
    fresh = update - jnp.einsum("hncd,hnde->hnce", correction, starts, precision=PRECISE)
    outputs = jnp.einsum("hncd,hnde->hnce", query_decay, starts, precision=PRECISE) + jnp.einsum(
        "hnij,hnje->hnie", scores, fresh, precision=PRECISE
    )
    raw_mix = outputs.transpose(1, 2, 0, 3).reshape(length, head_count, width)
    return (
        raw_mix * lax.rsqrt(jnp.mean(raw_mix * raw_mix, -1, keepdims=True) + EPSILON) * norm_gain
    ).astype(jnp.bfloat16)


def experts_body(ffn_input, ffn_gain, expert_ids, expert_share, w_gate, w_up, w_down):
    floats = ffn_input.astype(jnp.float32)
    square_sum = lax.psum(jnp.sum(floats * floats, -1), "tp")
    full_width = ffn_input.shape[1] * lax.axis_size("tp")
    normed = (floats * lax.rsqrt(square_sum / full_width + EPSILON)[:, None] * ffn_gain).astype(
        jnp.bfloat16
    )
    pick_count = expert_ids.shape[1]
    flat_ids = expert_ids.reshape(-1)
    sort_order = jnp.argsort(flat_ids, stable=True)
    source_rows = sort_order // pick_count
    experts_local = w_gate.shape[0]
    expert_devices = lax.axis_size("ep")
    capacity = flat_ids.shape[0] // (experts_local * expert_devices)
    outgoing = normed[source_rows].reshape(expert_devices, experts_local, capacity, normed.shape[1])
    arrived = lax.all_to_all(outgoing, "ep", split_axis=0, concat_axis=0, tiled=True)
    slab_in = lax.all_gather(arrived, "tp", axis=3, tiled=True)
    gate_sum = jnp.einsum("secl,elf->secf", slab_in, w_gate, preferred_element_type=jnp.float32)
    up_sum = jnp.einsum("secl,elf->secf", slab_in, w_up, preferred_element_type=jnp.float32)
    hidden = (jax.nn.silu(gate_sum) * up_sum).astype(jnp.bfloat16)
    merged = jnp.einsum(
        "secf,efd->secd",
        lax.all_gather(hidden, "tp", axis=3, tiled=True),
        w_down,
        preferred_element_type=jnp.float32,
    )
    copies = merged.astype(jnp.bfloat16)
    returned = lax.all_to_all(copies, "ep", split_axis=0, concat_axis=0, tiled=True).reshape(
        -1, w_down.shape[2]
    )
    slots = jnp.argsort(sort_order)
    per_slot = returned[slots].reshape(expert_ids.shape[0], pick_count, -1)
    return jnp.sum(per_slot.astype(jnp.float32) * expert_share[..., None], axis=1).astype(
        jnp.bfloat16
    )

def mm(a, b, dims=ROWS_COLS):
    return lax.dot_general(a, b, dims, preferred_element_type=F32)


def exact(a, b, dims=ROWS_COLS):
    return lax.dot_general(a, b, dims, preferred_element_type=F32, precision=PRECISE)


def halves(a):
    high = a.astype(BF16)
    return high, (a - high.astype(F32)).astype(BF16)


def joined(parts, dim):
    return jnp.concatenate(parts, dim)


def split(a):
    return joined(halves(a), 1)


def twice(b):
    return joined([b, b], 0)


def three(a, b):
    n = b.shape[1]
    bh, bl = halves(b)
    rhs = joined([joined([bh, bl], 1), joined([bh, jnp.zeros_like(bl)], 1)], 0)
    out = mm(split(a), rhs)
    return out[:, :n] + out[:, n:]


def iota(shape, dim):
    return lax.broadcasted_iota(jnp.int32, shape, dim)


def pair_rows(h, c, chunks):
    return (h % 2) * chunks + c


def state_pair(g, q_ref, k_ref, v_ref, rows_s, cols_s, gp_s, sc_s, wu_s, z_s, m_s, n_s, service):
    length = k_ref.shape[0]
    n = 128
    chunks = length // n
    count = 2 * chunks
    units = [(i, c) for i in range(2) for c in range(chunks)]
    row, col = iota((n, n), 0), iota((n, n), 1)
    causal, strict = row >= col, row > col
    same = (row >= n // 2) == (col >= n // 2)
    eye = (row == col).astype(F32)

    def block(ref, u):
        i, c = units[u]
        return ref[c * n : (c + 1) * n, pl.ds(pl.multiple_of((2 * g + i) * n, n), n)]

    def row_of(kind, u):
        return rows_s[g, kind * count + u : kind * count + u + 1, :]

    def col_of(kind, u):
        return cols_s[g, :, kind * count + u : kind * count + u + 1]

    everything = range(count)
    rks, gathered = [], jnp.zeros((n, n), F32)
    for u in everything:
        kf = block(k_ref, u).astype(F32)
        rk = lax.rsqrt(jnp.sum(kf * kf, -1, keepdims=True) + EPSILON)
        rks.append(rk)
        gathered = jnp.where(col == u, rk, gathered)
    rows_s[g, 2 * count : 3 * count, :] = jnp.transpose(gathered)[:count]
    prods, powers, offs, tails, rowsets = [], [], [], [], []
    for u in everything:
        i, c = units[u]
        k, q = block(k_ref, u), block(q_ref, u)
        qf = q.astype(F32)
        rq = lax.rsqrt(jnp.sum(qf * qf, -1, keepdims=True) + EPSILON) * (n ** (-0.5))
        crow, brow, rkrow = row_of(0, u), row_of(1, u), row_of(2, u)
        ccol, bcol = col_of(0, u), col_of(1, u)
        raw = mm(joined([k, q], 0), k, ROWS_ROWS)
        dm = jnp.where(causal, jnp.exp(jnp.where(causal, ccol - crow, 0.0)), 0.0) * rkrow
        lower = jnp.where(strict, raw[:n] * dm * (rks[u] * bcol), 0.0)
        sc_s[g, u] = split(raw[n:] * dm * rq)
        gp_s[g, u] = qf * (rq * jnp.exp(ccol))
        neg = jnp.where(same, -lower, 0.0)
        offs.append(jnp.where(same, 0.0, lower))
        prods.append(eye + neg)
        powers.append(neg)
        clast = crow[:, n - 1 :]
        tails.append((rks[u] * jnp.exp(clast - ccol), jnp.exp(clast)))
        rowsets.append((brow, brow * rkrow * jnp.exp(crow)))
    powers = [three(p, p) for p in powers]
    service(0)
    for turn in range((BLOCK - 1).bit_length() - 2):
        both = [three(joined([a, p], 0), p) for a, p in zip(prods, powers)]
        prods = [a + b[:n] for a, b in zip(prods, both)]
        powers = [b[n:] for b in both]
    service(1)
    prods = [a + three(a, p) for a, p in zip(prods, powers)]
    mids = [three(o, a) for o, a in zip(offs, prods)]
    prods = [a - three(a, m) for a, m in zip(prods, mids)]
    pairs = []
    for u in everything:
        k, v = block(k_ref, u), block(v_ref, u)
        x, w = prods[u] * rowsets[u][0], prods[u] * rowsets[u][1]
        pairs.append(joined([mm(split(w), twice(k)), mm(split(x), twice(v))], 1))
        wu_s[g, u] = pairs[u].astype(BF16)
    service(2)
    steps = []
    for u in everything:
        scale, last = tails[u]
        sh, sl = halves(pairs[u] * scale)
        k = block(k_ref, u)
        moved = mm(twice(k), joined([sh, sl], 0), COLS_COLS)
        steps.append((last * eye - moved[:, :n], moved[:, n:]))
    states = [None, None]
    for c in range(chunks):
        for i in range(2):
            step, add = steps[i * chunks + c]
            if c == 0:
                states[i] = joined([step, add], 1)
            else:
                z_s[g, i * (chunks - 1) + c - 1] = states[i].astype(BF16)
                sh, sl = halves(states[i])
                th, tl = halves(step)
                out = mm(joined([th, tl], 1), twice(sh)) + mm(th, sl)
                states[i] = out + joined([jnp.zeros_like(add), add], 1)
    for i in range(2):
        m_s[2 * g + i] = split(states[i][:, :n])
        n_s[2 * g + i] = states[i][:, n:]


def output_pair(g, gp_s, sc_s, wu_s, z_s, gs_s, y_s, chunks):
    n = 128
    count = 2 * chunks
    spreads = [mm(sc_s[g, u], twice(wu_s[g, u])) for u in range(count)]
    for u in range(count):
        i, c = u // chunks, u % chunks
        reader, base = gp_s[g, u] - spreads[u][:, :n], spreads[u][:, n:]
        if c > 0:
            both = mm(split(reader), twice(z_s[g, i * (chunks - 1) + c - 1]))
            reader, base = both[:, :n], both[:, n:] + base
        here = slice(c * n, (c + 1) * n)
        gs_s[2 * g + i, here, :] = split(reader)
        y_s[2 * g + i, here, :] = base


def layer_kernel(
    q_ref, k_ref, v_ref, beta_ref, decay_ref, ngain_ref, x_ref, gain_ref, ids_ref, share_ref,
    wg_ref, wu_ref, wd_ref, mix_ref, ffn_ref,
    q_s, k_s, v_s, flat_s, rows_s, cols_s, sc_s, wu_s, z_s, gp_s, gs_s, y_s, m_s, n_s, sin_s, sout_s,
    wg_v, wu_v, wd_v, perm_s, disp, info_out, info_all, gall, xall, xe, hmine, hall, place_s, back_s, wide_s, copies_s,
    ret_out, ret_in,
    w_sem, d_send, d_recv, i_send, i_recv, g_send, g_recv,
    gx_send, gx_recv, gc_send, gc_recv, hx_send, hx_recv, hc_send, hc_recv,
    r_send, r_recv, c_send, c_recv,
):
    ep, tp = lax.axis_size("ep"), lax.axis_size("tp")
    me, mt = lax.axis_index("ep"), lax.axis_index("tp")
    chips = tp // 2
    chip, core = mt // 2, lax.rem(mt, 2)
    mate = chip * 2 + 1 - core
    heads, length = beta_ref.shape
    tokens, dl = x_ref.shape
    local = wg_ref.shape[0]
    cap = tokens // ep
    cap_e = tokens * 2 // local
    parts = r_send.shape[1]
    wide_part = ffn_ref.shape[1] // parts

    def away(axis, count, mine, step):
        return {axis: lax.rem(mine + step, count)}

    def remote(src, dst, ssem, rsem, device):
        return pltpu.make_async_remote_copy(
            src_ref=src, dst_ref=dst, send_sem=ssem, recv_sem=rsem,
            device_id=device, device_id_type=MESH,
        )

    barrier = pltpu.get_barrier_semaphore()
    for step in range(1, ep):
        pl.semaphore_signal(barrier, inc=1, device_id=away("ep", ep, me, step), device_id_type=MESH)
    for step in range(1, tp):
        pl.semaphore_signal(barrier, inc=1, device_id=away("tp", tp, mt, step), device_id_type=MESH)

    def weight(which, e):
        src, dst = ((wg_ref, wg_v), (wu_ref, wu_v), (wd_ref, wd_v))[which]
        return pltpu.make_async_copy(src.at[e], dst.at[e], w_sem.at[which, e])

    for which in range(3):
        for e in range(local):
            weight(which, e).start()

    ids = ids_ref[...]
    first = ids[0:1]
    group = jnp.zeros_like(first)
    for d in range(1, ep):
        group = group + (first >= d * local).astype(jnp.int32)
    n_rows = info_out.shape[0]
    upper = (iota((tokens, tokens), 0) < iota((tokens, tokens), 1)).astype(F32).astype(BF16)
    g_rows = max(8, ep)
    member = (iota((g_rows, tokens), 0) == group).astype(F32)
    rank = jnp.sum(member * mm(member.astype(BF16), upper), 0, keepdims=True)
    slot = group.astype(F32) * cap + rank
    perm = (iota((tokens, tokens), 0).astype(F32) == slot).astype(F32)
    perm_s[...] = perm.astype(BF16)
    disp[...] = mm(perm.astype(BF16), x_ref[...]).astype(BF16)
    l0, l1 = ids[0:1] - group * local, ids[1:2] - group * local
    shares = share_ref[...]
    line = iota((n_rows, tokens), 0)
    picked = ((line == l0) | (line == l1)).astype(F32)
    shared = jnp.where(
        line - local == l0, shares[0:1], jnp.where(line - local == l1, shares[1:2], 0.0)
    )
    info = exact(jnp.where(line < local, picked, shared), perm, ROWS_ROWS)
    info_out[...] = info
    info_all[me] = info
    gall[mt] = gain_ref[...]
    xall[mt, pl.ds(pl.multiple_of(me * cap, cap), cap), :] = disp[
        pl.ds(pl.multiple_of(me * cap, cap), cap), :
    ]

    def dispatch(step):
        to = lax.rem(me + step, ep)
        return remote(
            disp.at[pl.ds(pl.multiple_of(to * cap, cap), cap)],
            xall.at[mt, pl.ds(pl.multiple_of(me * cap, cap), cap)],
            d_send.at[to], d_recv.at[me], {"ep": to},
        )

    def tell(step):
        to = lax.rem(me + step, ep)
        return remote(info_out, info_all.at[me], i_send.at[to], i_recv.at[me], {"ep": to})

    def gains(step):
        to = lax.rem(mt + step, tp)
        return remote(gain_ref, gall.at[mt], g_send.at[to], g_recv.at[mt], {"tp": to})

    def chunk_of(origin, s):
        return xall.at[origin, pl.ds(pl.multiple_of(s * cap, cap), cap)]

    def over_x(step, s):
        to = lax.rem(chip + step, chips)
        part = chunk_of(mt, s)
        return remote(part, part, gx_send.at[to, s], gx_recv.at[chip, s], {"tp": to * 2 + core})

    def to_mate(step, s):
        origin = lax.rem(chip + step, chips)
        part = chunk_of(origin * 2 + core, s)
        return remote(part, part, gc_send.at[origin, s], gc_recv.at[origin, s], {"tp": mate})

    def expert_rows(e):
        return pl.ds(pl.multiple_of(e * cap_e, cap_e), cap_e)

    def h_over_x(step, e):
        to = lax.rem(chip + step, chips)
        return remote(
            hmine.at[expert_rows(e)], hall.at[mt, expert_rows(e)],
            hx_send.at[to, e], hx_recv.at[chip, e], {"tp": to * 2 + core},
        )

    def h_to_mate(step, e):
        origin = lax.rem(chip + step, chips)
        part = hall.at[origin * 2 + core, expert_rows(e)]
        src = hmine.at[expert_rows(e)] if step == 0 else part
        return remote(src, part, hc_send.at[origin, e], hc_recv.at[origin, e], {"tp": mate})

    def h_relay(e):
        for step in range(1, chips):
            origin = lax.rem(chip + step, chips)
            landed(hall.at[origin * 2 + core, expert_rows(e)], hx_recv.at[origin, e])
            h_to_mate(step, e).start()

    def giving(step, part):
        to = lax.rem(me + step, ep)
        lanes = slice(part * wide_part, (part + 1) * wide_part)
        return remote(
            ret_out.at[pl.ds(pl.multiple_of(to * cap, cap), cap), lanes],
            ret_in.at[pl.ds(pl.multiple_of(me * cap, cap), cap), lanes],
            r_send.at[to, part], r_recv.at[me, part], {"ep": to},
        )

    def landed(dst, sem):
        pltpu.make_async_copy(dst, dst, sem).wait()

    pl.semaphore_wait(barrier, ep - 1 + tp - 1)
    for step in range(1, ep):
        dispatch(step).start()
        tell(step).start()
    for step in range(1, tp):
        gains(step).start()

    def forward(j):
        s = lax.rem(me + j, ep)
        if j > 0:
            landed(chunk_of(mt, s), d_recv.at[s])
        for step in range(1, chips):
            over_x(step, s).start()
        to_mate(0, s).start()

    def relay(j):
        s = lax.rem(me + j, ep)
        for step in range(1, chips):
            origin = lax.rem(chip + step, chips)
            landed(chunk_of(origin * 2 + core, s), gx_recv.at[origin, s])
            to_mate(step, s).start()

    order = [j for near in range(1, ep // 2 + 1) for j in sorted({near, ep - near})]
    forward(0)

    for src, dst in ((k_ref, k_s), (v_ref, v_s), (q_ref, q_s)):
        flat_s[...] = src[...].astype(F32)
        for h in range(heads):
            for c in range(length // 128):
                dst[c * 128 : (c + 1) * 128, h * 128 : (h + 1) * 128] = flat_s[
                    pl.ds(c * 128 * heads + h, 128, stride=heads), :
                ].astype(BF16)

    strengths = 1.0 / (1.0 + jnp.exp(-beta_ref[...]))
    raw = decay_ref[...]
    small = jnp.exp(-jnp.abs(raw))
    bigger = 1.0 + small
    diff = bigger - 1.0
    log_term = jnp.where(
        diff == 0.0, small, jnp.log(bigger) * small / jnp.where(diff == 0.0, 1.0, diff)
    )
    rates = jnp.maximum(raw, 0.0) + log_term
    ones_upper = (iota((128, 128), 0) <= iota((128, 128), 1)).astype(F32)
    chunks = length // 128
    rows_s[...] = jnp.zeros_like(rows_s)
    for c in range(chunks):
        here = slice(c * 128, (c + 1) * 128)
        summed = -exact(rates[:, here], ones_upper)
        for h in range(heads):
            u = pair_rows(h, c, chunks)
            rows_s[h // 2, u : u + 1, :] = summed[h : h + 1]
            rows_s[h // 2, 2 * chunks + u : 2 * chunks + u + 1, :] = strengths[h : h + 1, here]
    for g in range(heads // 2):
        cols_s[g] = jnp.transpose(rows_s[g])

    def chain_copy(h):
        return remote(sout_s.at[h], sin_s.at[h], c_send.at[h], c_recv.at[h], {"ep": lax.rem(me + 1, ep)})

    def one_pair(g, carry):
        def service(place):
            if place == 1:
                @pl.when(g == 0)
                def _():
                    for j in order[:-1]:
                        forward(j)

                @pl.when(g == 1)
                def _():
                    for j in order[:-1]:
                        relay(j)

        state_pair(g, q_s, k_s, v_s, rows_s, cols_s, gp_s, sc_s, wu_s, z_s, m_s, n_s, service)

        @pl.when(me == 0)
        def _():
            for i in range(2):
                sout_s[2 * g + i] = n_s[2 * g + i].astype(BF16)
                chain_copy(2 * g + i).start()

        @pl.when(g == 0)
        def _():
            relay(0)
            forward(order[-1])

        return carry

    lax.fori_loop(0, heads // 2, one_pair, 0)
    relay(order[-1])

    def chain_turn(low, high):
        def turn(h, carry):
            landed(sin_s.at[h], c_recv.at[h])

            @pl.when(me < ep - 1)
            def _():
                sout_s[h] = (mm(m_s[h], twice(sin_s[h])) + n_s[h]).astype(BF16)
                chain_copy(h).start()

            return carry

        def all_turns():
            lax.fori_loop(low, high, turn, 0)

        return all_turns

    def outputs(low, high):
        def one(h, carry):
            output_pair(h, gp_s, sc_s, wu_s, z_s, gs_s, y_s, chunks)
            return carry

        lax.fori_loop(low, high, one, 0)

    last = heads - 1
    pl.when(me == 1)(chain_turn(0, last))

    for step in range(1, ep):
        s = lax.rem(me + step, ep)
        landed(info_all.at[s], i_recv.at[s])
    r_in, r_out = iota((tokens, tokens), 0), iota((tokens, tokens), 1)
    told = jnp.zeros((n_rows, tokens), F32)
    for s in range(ep):
        take = (r_in - me * cap == r_out - s * cap) & (r_out >= s * cap) & (r_out < (s + 1) * cap)
        told = told + exact(info_all[s], take.astype(F32))
    ranks = mm(told.astype(BF16), upper)
    for e in range(local):
        where_to = iota((cap_e, tokens), 0).astype(F32) == ranks[e : e + 1]
        placed = jnp.where(where_to, told[e : e + 1], 0.0)
        place_s[e * cap_e : (e + 1) * cap_e, :] = placed.astype(BF16)
        left = jnp.transpose(placed * told[local + e : local + e + 1])
        for piece in range(back_s.shape[0]):
            taken = left.astype(BF16)
            back_s[piece, :, e * cap_e : (e + 1) * cap_e] = taken
            left = left - taken.astype(F32)

    for step in range(1, tp):
        t = lax.rem(mt + step, tp)
        landed(gall.at[t], g_recv.at[t])
    for step in range(chips):
        origin = lax.rem(chip + step, chips)
        for s in range(ep):
            landed(chunk_of(origin * 2 + 1 - core, s), gc_recv.at[origin, s])

    def squares(t, total):
        part = xall[t].astype(F32)
        return total + jnp.sum(part * part, -1, keepdims=True)

    total = lax.fori_loop(0, tp, squares, jnp.zeros((tokens, 1), F32))
    scale = lax.rsqrt(total / (tp * dl) + EPSILON)

    def spread_rows(t, carry):
        normed = (xall[t].astype(F32) * scale * gall[t]).astype(BF16)
        xe[:, pl.ds(pl.multiple_of(t * dl, dl), dl)] = mm(place_s[...], normed).astype(BF16)
        return carry

    lax.fori_loop(0, tp, spread_rows, 0)

    def one_expert(e, carry):
        rows = pl.ds(pl.multiple_of(e * cap_e, cap_e), cap_e)
        weight(0, e).wait()
        weight(1, e).wait()
        gate = mm(xe[rows, :], wg_v[e])
        up = mm(xe[rows, :], wu_v[e])
        hidden = (gate / (1.0 + jnp.exp(-gate)) * up).astype(BF16)
        hmine[rows, :] = hidden
        hall[mt, rows, :] = hidden
        for step in range(1, chips):
            h_over_x(step, e).start()
        h_to_mate(0, e).start()
        return carry

    lax.fori_loop(0, local, one_expert, 0)
    h_relay(0)
    pl.when(me == 1)(chain_turn(last, heads))
    pl.when(me == 2)(chain_turn(0, last))
    outputs(0, 1)
    for e in range(1, local):
        h_relay(e)
    pl.when(me == 2)(chain_turn(last, heads))
    pl.when(me >= 3)(chain_turn(0, last))
    for e in range(local):
        for step in range(chips):
            origin = lax.rem(chip + step, chips)
            landed(hall.at[origin * 2 + 1 - core, expert_rows(e)], hc_recv.at[origin, e])

    for e in range(local):
        weight(2, e).wait()
    own = pl.ds(pl.multiple_of(me * cap, cap), cap)
    for t in range(tp):
        wide_s[:, t * hall.shape[2] : (t + 1) * hall.shape[2]] = hall[t]
    for part in range(parts):
        lanes = slice(part * wide_part, (part + 1) * wide_part)
        for e in range(local):
            rows = slice(e * cap_e, (e + 1) * cap_e)
            copies_s[rows, lanes] = mm(wide_s[rows, :], wd_v[e, :, lanes]).astype(BF16)
        result = mm(back_s[0], copies_s[:, lanes])
        for piece in range(1, back_s.shape[0]):
            result = result + mm(back_s[piece], copies_s[:, lanes])
        ret_out[:, lanes] = result.astype(BF16)
        ret_in[own, lanes] = ret_out[own, lanes]
        for step in range(1, ep):
            giving(step, part).start()

    outputs(1, heads // 2)
    pl.when(me >= 3)(chain_turn(last, heads))

    @pl.when(me == 0)
    def _():
        sin_s[...] = jnp.zeros_like(sin_s)

    for h in range(heads):
        mixed = mm(gs_s[h], twice(sin_s[h])) + y_s[h]
        normed = mixed * lax.rsqrt(jnp.mean(mixed * mixed, -1, keepdims=True) + EPSILON)
        flat_s[pl.ds(h, length, stride=heads), :] = normed * ngain_ref[...]
    mix_ref[...] = flat_s[...].astype(BF16)

    for step in range(1, ep):
        s = lax.rem(me + step, ep)
        for part in range(parts):
            lanes = slice(part * wide_part, (part + 1) * wide_part)
            landed(ret_in.at[pl.ds(pl.multiple_of(s * cap, cap), cap), lanes], r_recv.at[s, part])
    ffn_ref[...] = mm(perm_s[...], ret_in[...], COLS_COLS).astype(BF16)

    for step in range(1, ep):
        dispatch(step).wait_send()
        tell(step).wait_send()
        for part in range(parts):
            giving(step, part).wait_send()
    for step in range(1, tp):
        gains(step).wait_send()
    for step in range(1, chips):
        for e in range(local):
            h_over_x(step, e).wait_send()
        for s in range(ep):
            over_x(step, s).wait_send()
    for step in range(chips):
        for e in range(local):
            h_to_mate(step, e).wait_send()
        for s in range(ep):
            to_mate(step, s).wait_send()

    @pl.when(me < ep - 1)
    def _():
        def sent(h, carry):
            chain_copy(h).wait_send()
            return carry

        lax.fori_loop(0, heads, sent, 0)


def hand_on(mix_ref, ffn_ref, mix_out, ffn_out):
    mix_out[...] = mix_ref[...]
    ffn_out[...] = ffn_ref[...]


def fused_body(
    mix_query, mix_keys, mix_values, beta_in, decay_in, norm_gain, ffn_input, ffn_gain,
    expert_ids, expert_share, w_gate, w_up, w_down,
):
    ep, tp = lax.axis_size("ep"), lax.axis_size("tp")
    length, heads, width = mix_query.shape
    tokens, dl = ffn_input.shape
    local, full, fl = w_gate.shape
    out_width = w_down.shape[2]
    picks = expert_ids.shape[1]
    n_rows = max(8, 2 * local)
    chips = tp // 2
    rows_e = tokens * picks
    parts = max(1, min(2, out_width // 512))
    dma = pltpu.SemaphoreType.DMA
    vmem = pl.BlockSpec(memory_space=pltpu.VMEM)
    hbm = pl.BlockSpec(memory_space=pl.ANY)
    pairs, chunks = heads // 2, length // width
    mix_out, ffn_out = pl.pallas_call(
        layer_kernel,
        out_shape=(
            jax.ShapeDtypeStruct((length * heads, width), BF16),
            jax.ShapeDtypeStruct((tokens, out_width), BF16),
        ),
        in_specs=[vmem] * 10 + [hbm] * 3,
        out_specs=(vmem, vmem),
        scratch_shapes=[
            pltpu.VMEM((length, heads * width), BF16),
            pltpu.VMEM((length, heads * width), BF16),
            pltpu.VMEM((length, heads * width), BF16),
            pltpu.VMEM((length * heads, width), F32),
            pltpu.VMEM((pairs, 128, 128), F32),
            pltpu.VMEM((pairs, 128, 128), F32),
            pltpu.VMEM((pairs, 2 * chunks, width, 2 * width), BF16),
            pltpu.VMEM((pairs, 2 * chunks, width, 2 * width), BF16),
            pltpu.VMEM((pairs, max(2 * (chunks - 1), 1), width, 2 * width), BF16),
            pltpu.VMEM((pairs, 2 * chunks, width, width), F32),
            pltpu.VMEM((heads, length, 2 * width), BF16),
            pltpu.VMEM((heads, length, width), F32),
            pltpu.VMEM((heads, width, 2 * width), BF16),
            pltpu.VMEM((heads, width, width), F32),
            pltpu.VMEM((heads, width, width), BF16),
            pltpu.VMEM((heads, width, width), BF16),
            pltpu.VMEM(w_gate.shape, BF16),
            pltpu.VMEM(w_up.shape, BF16),
            pltpu.VMEM(w_down.shape, BF16),
            pltpu.VMEM((tokens, tokens), BF16),
            pltpu.VMEM((tokens, dl), BF16),
            pltpu.VMEM((n_rows, tokens), F32),
            pltpu.VMEM((ep, n_rows, tokens), F32),
            pltpu.VMEM((tp, 1, dl), F32),
            pltpu.VMEM((tp, tokens, dl), BF16),
            pltpu.VMEM((rows_e, full), BF16),
            pltpu.VMEM((rows_e, fl), BF16),
            pltpu.VMEM((tp, rows_e, fl), BF16),
            pltpu.VMEM((rows_e, tokens), BF16),
            pltpu.VMEM((3, tokens, rows_e), BF16),
            pltpu.VMEM((rows_e, tp * fl), BF16),
            pltpu.VMEM((rows_e, out_width), BF16),
            pltpu.VMEM((tokens, out_width), BF16),
            pltpu.VMEM((tokens, out_width), BF16),
            dma((3, local)),
            dma((ep,)), dma((ep,)), dma((ep,)), dma((ep,)),
            dma((tp,)), dma((tp,)),
            dma((chips, ep)), dma((chips, ep)), dma((chips, ep)), dma((chips, ep)),
            dma((chips, local)), dma((chips, local)), dma((chips, local)), dma((chips, local)),
            dma((ep, parts)), dma((ep, parts)),
            dma((heads,)), dma((heads,)),
        ],
        compiler_params=pltpu.CompilerParams(
            collective_id=0, has_side_effects=True, vmem_limit_bytes=60 * 1024 * 1024
        ),
    )(
        mix_query.reshape(length * heads, width),
        mix_keys.reshape(length * heads, width),
        mix_values.reshape(length * heads, width),
        beta_in, decay_in, norm_gain.reshape(1, width),
        ffn_input, ffn_gain.reshape(1, dl), expert_ids.T, expert_share.T,
        w_gate, w_up, w_down,
    )
    mix_out, ffn_out = pl.pallas_call(
        hand_on,
        out_shape=(
            jax.ShapeDtypeStruct(mix_out.shape, BF16),
            jax.ShapeDtypeStruct(ffn_out.shape, BF16),
        ),
        in_specs=[vmem] * 2,
        out_specs=(vmem, vmem),
        cost_estimate=pl.CostEstimate(flops=1000, bytes_accessed=2**21, transcendentals=0),
    )(mix_out, ffn_out)
    return (mix_out.reshape(length, heads, width), ffn_out)


def body(
    mix_query,
    mix_keys,
    mix_values,
    beta_in,
    decay_in,
    norm_gain,
    ffn_input,
    ffn_gain,
    expert_ids,
    expert_share,
    w_gate,
    w_up,
    w_down,
):
    width, local = mix_query.shape[2], w_gate.shape[0]
    whole_groups = local % GROUP == 0 and expert_ids.shape[1] == 2
    even = lax.axis_size("tp") % 2 == 0 and lax.axis_size("tp") > 1 and lax.axis_size("ep") > 1
    if whole_groups and even and mix_query.shape[1] == 4 and width == 128 and mix_query.shape[0] % 128 == 0:
        return fused_body(
            mix_query,
            mix_keys,
            mix_values,
            beta_in,
            decay_in,
            norm_gain,
            ffn_input,
            ffn_gain,
            expert_ids,
            expert_share,
            w_gate,
            w_up,
            w_down,
        )
    mix_out = mixer_body(mix_query, mix_keys, mix_values, beta_in, decay_in, norm_gain)
    ffn_out = experts_body(ffn_input, ffn_gain, expert_ids, expert_share, w_gate, w_up, w_down)
    return (mix_out, ffn_out)


def solution(mesh):
    placed = (
        P(("grp", "ep"), "tp", None),
        P(("grp", "ep"), "tp", None),
        P(("grp", "ep"), "tp", None),
        P("tp", ("grp", "ep")),
        P("tp", ("grp", "ep")),
        P(),
        P(("grp", "ep"), "tp"),
        P("tp"),
        P(("grp", "ep"), None),
        P(("grp", "ep"), None),
        P("ep", None, "tp"),
        P("ep", None, "tp"),
        P("ep", None, "tp"),
    )
    return jax.shard_map(
        body,
        mesh=mesh,
        in_specs=placed,
        out_specs=(P(("grp", "ep"), "tp", None), P(("grp", "ep"), "tp")),
        check_vma=False,
    )
```

```python
import functools
import jax
import jax.numpy as jnp
from jax import lax
from jax.experimental import pallas as pl
from jax.experimental.pallas import tpu as pltpu
from jax.sharding import PartitionSpec as P

BLOCK = 64
GROUP = 4
F32 = jnp.float32
BF16 = jnp.bfloat16
MESH = pl.DeviceIdType.MESH
ROWS_COLS = (((1,), (0,)), ((), ()))
ROWS_ROWS = (((1,), (1,)), ((), ()))
COLS_COLS = (((0,), (0,)), ((), ()))


PRECISE = lax.Precision.HIGHEST
EPSILON = 1e-06


def entering_2(value, axis, join, neutral):
    count, mine = (lax.axis_size(axis), lax.axis_index(axis))
    pieces = jax.tree.map(lambda part: lax.all_gather(part, axis), value)
    subtotal = jax.tree.map(
        lambda part, zero: jnp.full_like(part, 0) + jnp.asarray(zero, part.dtype), value, neutral
    )

    def turn(position, subtotal):
        longer = join(subtotal, jax.tree.map(lambda part: part[position], pieces))
        return jax.tree.map(lambda new, old: jnp.where(position < mine, new, old), longer, subtotal)

    return lax.fori_loop(0, count - 1, turn, subtotal)


def unit_inverse(strict_lower):
    extent = strict_lower.shape[-1]
    identity = jnp.eye(extent, dtype=jnp.float32)
    powered = -strict_lower
    product = identity + powered
    for section_index in range(1, (extent - 1).bit_length()):
        powered = jnp.matmul(powered, powered, precision=PRECISE)
        product = jnp.matmul(product, identity + powered, precision=PRECISE)
    return product


def block_terms(queries, keyset, valueset, betas, rates):
    extent = queries.shape[-2]
    cumulative = -jnp.cumsum(rates, axis=-1)
    positions = jnp.arange(extent)
    causal = positions[:, None] >= positions[None, :]
    strict = positions[:, None] > positions[None, :]
    spread = cumulative[..., :, None] - cumulative[..., None, :]
    decay_mask = jnp.where(causal, jnp.exp(jnp.where(causal, spread, 0.0)), 0.0)
    keys_beta = keyset * betas[..., None]
    values_beta = valueset * betas[..., None]
    lower_part = jnp.where(
        strict,
        jnp.einsum("...id,...jd->...ij", keys_beta, keyset, precision=PRECISE) * decay_mask,
        0.0,
    )
    inverse = unit_inverse(lower_part)
    update = jnp.einsum("...ij,...jd->...id", inverse, values_beta, precision=PRECISE)
    correction = jnp.einsum(
        "...ij,...jd->...id", inverse, keys_beta * jnp.exp(cumulative)[..., None], precision=PRECISE
    )
    scores = jnp.where(
        causal,
        jnp.einsum("...id,...jd->...ij", queries, keyset, precision=PRECISE) * decay_mask,
        0.0,
    )
    query_decay = queries * jnp.exp(cumulative)[..., None]
    key_decay = keyset * jnp.exp(cumulative[..., -1:] - cumulative)[..., None]
    block_decay = jnp.exp(cumulative[..., -1])
    return (query_decay, key_decay, update, correction, scores, block_decay)


def unit_rows(values_in, factor):
    floats = values_in.astype(jnp.float32)
    return floats * lax.rsqrt(jnp.sum(floats * floats, -1, keepdims=True) + EPSILON) * factor


def compose(earlier, later):
    return (
        jnp.matmul(later[0], earlier[0], precision=PRECISE),
        jnp.matmul(later[0], earlier[1], precision=PRECISE) + later[1],
    )


def mixer_body(mix_query, mix_keys, mix_values, beta_in, decay_in, norm_gain):
    length, head_count, width = mix_query.shape
    blocks = length // BLOCK

    def to_blocks(tensor):
        return tensor.reshape(blocks, BLOCK, head_count, width).transpose(2, 0, 1, 3)

    queries = to_blocks(unit_rows(mix_query, width ** (-0.5)))
    keyset = to_blocks(unit_rows(mix_keys, 1.0))
    valueset = to_blocks(mix_values.astype(jnp.float32))
    betas = jax.nn.sigmoid(beta_in).reshape(head_count, blocks, BLOCK)
    rates = jax.nn.softplus(decay_in).reshape(head_count, blocks, BLOCK)
    query_decay, key_decay, update, correction, scores, block_decay = block_terms(
        queries, keyset, valueset, betas, rates
    )
    identity = jnp.eye(width, dtype=jnp.float32)
    transfer = block_decay[..., None, None] * identity - jnp.einsum(
        "hncd,hnce->hnde", key_decay, correction, precision=PRECISE
    )
    offset = jnp.einsum("hncd,hnce->hnde", key_decay, update, precision=PRECISE)
    prefix_map, prefix_add = lax.associative_scan(compose, (transfer, offset), axis=1)
    total_map = prefix_map[:, -1]
    total_add = prefix_add[:, -1]
    empty_state = jnp.zeros((head_count, width, width), jnp.float32)
    unit_maps = jnp.broadcast_to(identity, (head_count, width, width))
    ignored_map, entering = entering_2(
        (total_map, total_add), "ep", compose, (unit_maps, empty_state)
    )
    after_blocks = jnp.matmul(prefix_map, entering[:, None], precision=PRECISE) + prefix_add
    starts = jnp.concatenate([entering[:, None], after_blocks[:, :-1]], axis=1)
    fresh = update - jnp.einsum("hncd,hnde->hnce", correction, starts, precision=PRECISE)
    outputs = jnp.einsum("hncd,hnde->hnce", query_decay, starts, precision=PRECISE) + jnp.einsum(
        "hnij,hnje->hnie", scores, fresh, precision=PRECISE
    )
    raw_mix = outputs.transpose(1, 2, 0, 3).reshape(length, head_count, width)
    return (
        raw_mix * lax.rsqrt(jnp.mean(raw_mix * raw_mix, -1, keepdims=True) + EPSILON) * norm_gain
    ).astype(jnp.bfloat16)


def experts_body(ffn_input, ffn_gain, expert_ids, expert_share, w_gate, w_up, w_down):
    floats = ffn_input.astype(jnp.float32)
    square_sum = lax.psum(jnp.sum(floats * floats, -1), "tp")
    full_width = ffn_input.shape[1] * lax.axis_size("tp")
    normed = (floats * lax.rsqrt(square_sum / full_width + EPSILON)[:, None] * ffn_gain).astype(
        jnp.bfloat16
    )
    pick_count = expert_ids.shape[1]
    flat_ids = expert_ids.reshape(-1)
    sort_order = jnp.argsort(flat_ids, stable=True)
    source_rows = sort_order // pick_count
    experts_local = w_gate.shape[0]
    expert_devices = lax.axis_size("ep")
    capacity = flat_ids.shape[0] // (experts_local * expert_devices)
    outgoing = normed[source_rows].reshape(expert_devices, experts_local, capacity, normed.shape[1])
    arrived = lax.all_to_all(outgoing, "ep", split_axis=0, concat_axis=0, tiled=True)
    slab_in = lax.all_gather(arrived, "tp", axis=3, tiled=True)
    gate_sum = jnp.einsum("secl,elf->secf", slab_in, w_gate, preferred_element_type=jnp.float32)
    up_sum = jnp.einsum("secl,elf->secf", slab_in, w_up, preferred_element_type=jnp.float32)
    hidden = (jax.nn.silu(gate_sum) * up_sum).astype(jnp.bfloat16)
    merged = jnp.einsum(
        "secf,efd->secd",
        lax.all_gather(hidden, "tp", axis=3, tiled=True),
        w_down,
        preferred_element_type=jnp.float32,
    )
    copies = merged.astype(jnp.bfloat16)
    returned = lax.all_to_all(copies, "ep", split_axis=0, concat_axis=0, tiled=True).reshape(
        -1, w_down.shape[2]
    )
    slots = jnp.argsort(sort_order)
    per_slot = returned[slots].reshape(expert_ids.shape[0], pick_count, -1)
    return jnp.sum(per_slot.astype(jnp.float32) * expert_share[..., None], axis=1).astype(
        jnp.bfloat16
    )

def mm(a, b, dims=ROWS_COLS):
    return lax.dot_general(a, b, dims, preferred_element_type=F32)


def exact(a, b, dims=ROWS_COLS):
    return lax.dot_general(a, b, dims, preferred_element_type=F32, precision=PRECISE)


def halves(a):
    high = a.astype(BF16)
    return high, (a - high.astype(F32)).astype(BF16)


def joined(parts, dim):
    return jnp.concatenate(parts, dim)


def split(a):
    return joined(halves(a), 1)


def twice(b):
    return joined([b, b], 0)


def three(a, b):
    n = b.shape[1]
    bh, bl = halves(b)
    rhs = joined([joined([bh, bl], 1), joined([bh, jnp.zeros_like(bl)], 1)], 0)
    out = mm(split(a), rhs)
    return out[:, :n] + out[:, n:]


def iota(shape, dim):
    return lax.broadcasted_iota(jnp.int32, shape, dim)


def unit_tools(heads, chunks, rows_s, cols_s):
    n = 128
    count = heads * chunks

    def block(ref, u):
        i, c = u // chunks, u % chunks
        return ref[c * n : (c + 1) * n, i * n : (i + 1) * n]

    def row_of(kind, u):
        return rows_s[kind * count + u : kind * count + u + 1, :]

    def col_of(kind, u):
        return cols_s[:, kind * count + u : kind * count + u + 1]

    return block, row_of, col_of


CUM, BETA, DECAY, SUMS, ROOT = range(5)


def solve_all(q_ref, k_ref, rows_s, cols_s, qd_s, sc_s, inv_s, service):
    n = 128
    heads, chunks = k_ref.shape[1] // n, k_ref.shape[0] // n
    count = heads * chunks
    row, col = iota((n, n), 0), iota((n, n), 1)
    causal, strict = row >= col, row > col
    same = (row >= n // 2) == (col >= n // 2)
    inside, outside = strict & same, strict & jnp.logical_not(same)
    diagonal = row == col
    eye = diagonal.astype(F32)
    block, row_of, col_of = unit_tools(heads, chunks, rows_s, cols_s)
    everything = range(count)
    cum = rows_s[:count, :]
    rows_s[DECAY * count : (DECAY + 1) * count, :] = jnp.exp(cum)
    based = cum - jnp.log(rows_s[count : 2 * count, :])
    cols_s[...] = jnp.transpose(joined([cum, jnp.zeros((n - count, n), F32)], 0))
    raws = []
    for u in everything:
        k = block(k_ref, u)
        raws.append(mm(joined([k, block(q_ref, u)], 0), k, ROWS_ROWS))
    prods, powers, offs = [], [], []
    for u in everything:
        raw, ccol = raws[u], col_of(CUM, u)
        total = jnp.sum(jnp.where(diagonal, raw[:n], 0.0), 0, keepdims=True) + EPSILON
        rows_s[SUMS * count + u : SUMS * count + u + 1, :] = total
        dm = jnp.exp(ccol - (based[u : u + 1] + jnp.log(total)))
        sc_s[u] = split(jnp.where(causal, raw[n:] * dm, 0.0))
        qd_s[u] = block(q_ref, u).astype(F32) * jnp.exp(ccol)
        minus = -raw[:n] * dm
        neg = jnp.where(inside, minus, 0.0)
        offs.append(jnp.where(outside, minus, 0.0))
        prods.append(eye + neg)
        powers.append(neg)
    service(0)
    powers = [three(p, p) for p in powers]
    for turn in range((BLOCK - 1).bit_length() - 2):
        both = [three(joined([a, p], 0), p) for a, p in zip(prods, powers)]
        prods = [a + b[:n] for a, b in zip(prods, both)]
        powers = [b[n:] for b in both]
    service(1)
    prods = [a + three(a, p) for a, p in zip(prods, powers)]
    mids = [three(o, a) for o, a in zip(offs, prods)]
    for u in everything:
        inv_s[u] = prods[u] + three(prods[u], mids[u])
    service(2)


def advanced(steps, adds, state):
    sh, sl = halves(state)
    th, tl = halves(steps)
    out = mm(joined([th, tl], 1), twice(sh)) + mm(th, sl)
    return out + joined([jnp.zeros_like(adds), adds], 1)


def carry_all(k_ref, v_ref, rows_s, cols_s, inv_s, sc_s, qd_s, y_s, z_s, m_s, n_s):
    n = 128
    heads, chunks = k_ref.shape[1] // n, k_ref.shape[0] // n
    count = heads * chunks
    eye = (iota((n, n), 0) == iota((n, n), 1)).astype(F32)
    block, row_of, col_of = unit_tools(heads, chunks, rows_s, cols_s)
    everything = range(count)
    totals, cum = rows_s[SUMS * count : (SUMS + 1) * count, :], rows_s[:count, :]
    rows_s[ROOT * count : (ROOT + 1) * count, :] = jnp.sqrt(totals)
    tail = rows_s[BETA * count : (BETA + 1) * count, :] / totals * jnp.exp(cum[:, n - 1 :] - cum)
    cols_s[...] = jnp.transpose(joined([tail, jnp.zeros((n - count, n), F32)], 0))
    pairs, steps, states, narrow = [], [], [], []
    for u in everything:
        k, v = block(k_ref, u), block(v_ref, u)
        solved = inv_s[u]
        x, w = solved * row_of(ROOT, u), solved * row_of(DECAY, u)
        pairs.append(joined([mm(split(w), twice(k)), mm(split(x), twice(v))], 1))
    for u in everything:
        narrow.append(pairs[u].astype(BF16))
        sh, sl = halves(pairs[u] * col_of(0, u))
        kt = jnp.transpose(block(k_ref, u).astype(F32)).astype(BF16)
        moved = mm(joined([kt, kt], 1), joined([sh, sl], 0))
        last = jnp.exp(row_of(CUM, u)[:, n - 1 :])
        steps.append((last * eye - moved[:, :n], moved[:, n:]))

    def spread_out(units):
        for u in units:
            spread = mm(sc_s[u], twice(narrow[u]))
            sc_s[u] = split(qd_s[u] - spread[:, :n])
            y_s[u] = spread[:, n:]

    def step_of(i, c):
        return steps[i * chunks + c]

    first = [joined(step_of(i, 0), 1) for i in range(heads)]
    if chunks == 4:
        second = [advanced(*step_of(i, 1), first[i]) for i in range(heads)]
        upper = [advanced(*step_of(i, 3), joined(step_of(i, 2), 1)) for i in range(heads)]
        spread_out(everything)
        third = [advanced(*step_of(i, 2), second[i]) for i in range(heads)]
        last = [advanced(upper[i][:, :n], upper[i][:, n:], second[i]) for i in range(heads)]
        states = [first, second, third, last]
    else:
        spread_out(everything)
        states = [first]
        for c in range(1, chunks):
            states.append([advanced(*step_of(i, c), states[-1][i]) for i in range(heads)])
    for i in range(heads):
        m_s[i] = split(states[-1][i][:, :n])
        n_s[i] = states[-1][i][:, n:]
        for c in range(chunks - 1):
            z_s[i * (chunks - 1) + c] = states[c][i].astype(BF16)


def outputs_all(heads, chunks, sc_s, z_s, y_s):
    n = 128
    for u in range(heads * chunks):
        i, c = u // chunks, u % chunks
        if c > 0:
            both = mm(sc_s[u], twice(z_s[i * (chunks - 1) + c - 1]))
            sc_s[u] = split(both[:, :n])
            y_s[u] = y_s[u] + both[:, n:]


def layer_kernel(
    q_hbm, k_hbm, v_hbm, beta_hbm, decay_hbm, ngain_hbm, x_hbm, gain_hbm, ids_hbm, share_hbm,
    wg_ref, wu_ref, wd_ref, mix_hbm, ffn_hbm,
    mix_ref, ffn_ref, out_sem,
    q_ref, k_ref, v_ref, beta_ref, decay_ref, ngain_ref, x_ref, gain_ref, ids_ref, share_ref, in_sem,
    q_s, k_s, v_s, flat_s, rows_s, cols_s, sc_s, z_s, qd_s, inv_s, y_s, m_s, n_s, sin_s, sout_s,
    wg_v, wu_v, wd_v, perm_s, disp, info_out, info_all, sq_all, sc_out, sc_all, gall, xall, xw_s, gacc_s, uacc_s, hmine, hall, place_s, back_s, dacc_s, copies_s,
    ret_out, ret_in,
    w_sem, d_send, d_recv, i_send, i_recv, g_send, g_recv, q_send, q_recv, t_send, t_recv,
    gx_send, gx_recv, gc_send, gc_recv, hx_send, hx_recv, hc_send, hc_recv,
    r_send, r_recv, c_send, c_recv,
):
    ep, tp = lax.axis_size("ep"), lax.axis_size("tp")
    me, mt = lax.axis_index("ep"), lax.axis_index("tp")
    chips = tp // 2
    chip, core = mt // 2, lax.rem(mt, 2)
    mate = chip * 2 + 1 - core
    heads, length = beta_ref.shape
    tokens, dl = x_ref.shape
    local = wg_ref.shape[0]
    cap = tokens // ep
    cap_e = tokens * 2 // local
    parts = r_send.shape[1]
    wide_part = ffn_ref.shape[1] // parts

    def nearest(k):
        left, right = me, ep - 1 - me
        inner = jnp.minimum(left, right)
        both = k < 2 * inner
        far = jnp.where(both, k // 2 + 1, k - inner + 1)
        upward = jnp.where(both, k % 2, jnp.where(right > left, 0, 1)) == 0
        return jnp.where(upward, me + far, me - far)

    def away(axis, count, mine, step):
        return {axis: lax.rem(mine + step, count)}

    def remote(src, dst, ssem, rsem, device):
        return pltpu.make_async_remote_copy(
            src_ref=src, dst_ref=dst, send_sem=ssem, recv_sem=rsem,
            device_id=device, device_id_type=MESH,
        )

    barrier = pltpu.get_barrier_semaphore()
    for step in range(1, ep):
        pl.semaphore_signal(barrier, inc=1, device_id=away("ep", ep, me, step), device_id_type=MESH)
    for step in range(1, tp):
        pl.semaphore_signal(barrier, inc=1, device_id=away("tp", tp, mt, step), device_id_type=MESH)

    def weight(which, e):
        src, dst = ((wg_ref, wg_v), (wu_ref, wu_v), (wd_ref, wd_v))[which]
        return pltpu.make_async_copy(src.at[e], dst.at[e], w_sem.at[which, e])

    arriving = [
        pltpu.make_async_copy(src, dst, in_sem.at[i])
        for i, (src, dst) in enumerate((
            (ids_hbm, ids_ref), (x_hbm, x_ref), (share_hbm, share_ref), (gain_hbm, gain_ref),
            (k_hbm, k_ref), (v_hbm, v_ref), (q_hbm, q_ref),
            (beta_hbm, beta_ref), (decay_hbm, decay_ref), (ngain_hbm, ngain_ref),
        ))
    ]
    for copy in arriving:
        copy.start()
    for copy in arriving[:4]:
        copy.wait()

    ids = ids_ref[...]
    first = ids[0:1]
    group = jnp.zeros_like(first)
    for d in range(1, ep):
        group = group + (first >= d * local).astype(jnp.int32)
    n_rows = info_out.shape[0]
    upper = (iota((tokens, tokens), 0) < iota((tokens, tokens), 1)).astype(F32).astype(BF16)
    g_rows = max(8, ep)
    member = (iota((g_rows, tokens), 0) == group).astype(F32)
    rank = jnp.sum(member * mm(member.astype(BF16), upper), 0, keepdims=True)
    slot = group.astype(F32) * cap + rank
    perm = (iota((tokens, tokens), 0).astype(F32) == slot).astype(F32)
    perm_s[...] = perm.astype(BF16)
    disp[...] = mm(perm.astype(BF16), x_ref[...]).astype(BF16)
    l0, l1 = ids[0:1] - group * local, ids[1:2] - group * local
    shares = share_ref[...]
    line = iota((n_rows, tokens), 0)
    picked = ((line == l0) | (line == l1)).astype(F32)
    shared = jnp.where(
        line - local == l0, shares[0:1], jnp.where(line - local == l1, shares[1:2], 0.0)
    )
    info = exact(jnp.where(line < local, picked, shared), perm, ROWS_ROWS)
    info_out[...] = info
    info_all[me] = info
    gall[mt] = gain_ref[...]
    sorted_rows = disp[...].astype(F32)
    sums = jnp.sum(sorted_rows * sorted_rows, -1, keepdims=True)
    sq_all[mt] = jnp.transpose(jnp.broadcast_to(sums, (tokens, tokens)))[:8]
    xall[mt, pl.ds(pl.multiple_of(me * cap, cap), cap), :] = disp[
        pl.ds(pl.multiple_of(me * cap, cap), cap), :
    ]

    def dispatch(step):
        to = nearest(step - 1)
        return remote(
            disp.at[pl.ds(pl.multiple_of(to * cap, cap), cap)],
            xall.at[mt, pl.ds(pl.multiple_of(me * cap, cap), cap)],
            d_send.at[to], d_recv.at[me], {"ep": to},
        )

    def tell(step):
        to = nearest(step - 1)
        return remote(info_out, info_all.at[me], i_send.at[to], i_recv.at[me], {"ep": to})

    def gains(step):
        to = lax.rem(mt + step, tp)
        return remote(gain_ref, gall.at[mt], g_send.at[to], g_recv.at[mt], {"tp": to})

    def squares(step):
        to = lax.rem(mt + step, tp)
        return remote(sq_all.at[mt], sq_all.at[mt], q_send.at[to], q_recv.at[mt], {"tp": to})

    def scales(step):
        to = nearest(step - 1)
        return remote(sc_out, sc_all.at[me], t_send.at[to], t_recv.at[me], {"ep": to})

    def send_scales():
        total = sq_all[mt]
        for step in range(1, tp):
            t = lax.rem(mt + step, tp)
            landed(sq_all.at[t], q_recv.at[t])
            total = total + sq_all[t]
        row = lax.rsqrt(total / (tp * dl) + EPSILON)
        sc_out[...] = row
        sc_all[me] = row
        for step in range(1, ep):
            scales(step).start()

    def chunk_of(origin, s):
        return xall.at[origin, pl.ds(pl.multiple_of(s * cap, cap), cap)]

    def over_x(step, s):
        to = lax.rem(chip + step, chips)
        part = chunk_of(mt, s)
        return remote(part, part, gx_send.at[to, s], gx_recv.at[chip, s], {"tp": to * 2 + core})

    def to_mate(step, s):
        origin = lax.rem(chip + step, chips)
        part = chunk_of(origin * 2 + core, s)
        return remote(part, part, gc_send.at[origin, s], gc_recv.at[origin, s], {"tp": mate})

    def expert_rows(e):
        return pl.ds(pl.multiple_of(e * cap_e, cap_e), cap_e)

    def h_over_x(step, e):
        to = lax.rem(chip + step, chips)
        return remote(
            hmine.at[expert_rows(e)], hall.at[mt, expert_rows(e)],
            hx_send.at[to, e], hx_recv.at[chip, e], {"tp": to * 2 + core},
        )

    def h_to_mate(step, e):
        origin = lax.rem(chip + step, chips)
        part = hall.at[origin * 2 + core, expert_rows(e)]
        src = hmine.at[expert_rows(e)] if step == 0 else part
        return remote(src, part, hc_send.at[origin, e], hc_recv.at[origin, e], {"tp": mate})

    def h_relay(e):
        for step in range(1, chips):
            origin = lax.rem(chip + step, chips)
            landed(hall.at[origin * 2 + core, expert_rows(e)], hx_recv.at[origin, e])
            h_to_mate(step, e).start()

    def giving(step, part):
        to = nearest(ep - 1 - step)
        lanes = slice(part * wide_part, (part + 1) * wide_part)
        return remote(
            ret_out.at[pl.ds(pl.multiple_of(to * cap, cap), cap), lanes],
            ret_in.at[pl.ds(pl.multiple_of(me * cap, cap), cap), lanes],
            r_send.at[to, part], r_recv.at[me, part], {"ep": to},
        )

    def landed(dst, sem):
        pltpu.make_async_copy(dst, dst, sem).wait()

    for copy in arriving[4:]:
        copy.wait()
    for which in range(3):
        for e in range(local):
            weight(which, e).start()

    pl.semaphore_wait(barrier, ep - 1 + tp - 1)
    for step in range(1, tp):
        squares(step).start()
    for step in range(1, ep):
        dispatch(step).start()
        tell(step).start()
    for step in range(1, tp):
        gains(step).start()

    def forward(j):
        s = nearest(j - 1) if j > 0 else me
        if j > 0:
            landed(chunk_of(mt, s), d_recv.at[s])
        for step in range(1, chips):
            over_x(step, s).start()
        to_mate(0, s).start()

    def relay(j):
        s = nearest(j - 1) if j > 0 else me
        for step in range(1, chips):
            origin = lax.rem(chip + step, chips)
            landed(chunk_of(origin * 2 + core, s), gx_recv.at[origin, s])
            to_mate(step, s).start()

    forward(0)

    for src, dst in ((k_ref, k_s), (v_ref, v_s), (q_ref, q_s)):
        flat_s[...] = src[...].astype(F32)
        for h in range(heads):
            for c in range(length // 128):
                dst[c * 128 : (c + 1) * 128, h * 128 : (h + 1) * 128] = flat_s[
                    pl.ds(c * 128 * heads + h, 128, stride=heads), :
                ].astype(BF16)

    strengths = 1.0 / (1.0 + jnp.exp(-beta_ref[...]))
    raw = decay_ref[...]
    small = jnp.exp(-jnp.abs(raw))
    bigger = 1.0 + small
    diff = bigger - 1.0
    log_term = jnp.where(
        diff == 0.0, small, jnp.log(bigger) * small / jnp.where(diff == 0.0, 1.0, diff)
    )
    rates = jnp.maximum(raw, 0.0) + log_term
    ones_upper = (iota((128, 128), 0) <= iota((128, 128), 1)).astype(F32)
    chunks = length // 128
    rows_s[...] = jnp.zeros_like(rows_s)
    for c in range(chunks):
        here = slice(c * 128, (c + 1) * 128)
        summed = -exact(rates[:, here], ones_upper)
        for h in range(heads):
            u = h * chunks + c
            rows_s[u : u + 1, :] = summed[h : h + 1]
            rows_s[heads * chunks + u : heads * chunks + u + 1, :] = strengths[h : h + 1, here]

    def chain_copy(h):
        return remote(sout_s.at[h], sin_s.at[h], c_send.at[h], c_recv.at[h], {"ep": lax.rem(me + 1, ep)})

    def carry_on():
        carry_all(k_s, v_s, rows_s, cols_s, inv_s, sc_s, qd_s, y_s, z_s, m_s, n_s)

        @pl.when(me == 0)
        def _():
            for h in range(heads):
                sout_s[h] = n_s[h].astype(BF16)
                chain_copy(h).start()

    def chain_turn(low, high):
        def turn(h, carry):
            landed(sin_s.at[h], c_recv.at[h])

            @pl.when(me < ep - 1)
            def _():
                sout_s[h] = (mm(m_s[h], twice(sin_s[h])) + n_s[h]).astype(BF16)
                chain_copy(h).start()

            return carry

        def all_turns():
            lax.fori_loop(low, high, turn, 0)

        return all_turns

    def outputs():
        outputs_all(heads, length // 128, sc_s, z_s, y_s)

    def early(place):
        if place == 0:
            send_scales()
        elif place == 1:
            for j in range(1, ep - 1):
                forward(j)
        elif place == 2:
            forward(ep - 1)
            relay(0)

    solve_all(q_s, k_s, rows_s, cols_s, qd_s, sc_s, inv_s, early)
    carry_on()
    for j in range(1, ep - 1):
        relay(j)

    for step in range(1, ep):
        s = lax.rem(me + step, ep)
        landed(info_all.at[s], i_recv.at[s])
    r_in, r_out = iota((ep * tokens, tokens), 0), iota((ep * tokens, tokens), 1)
    source = r_in // tokens
    takes = (r_in - source * tokens - me * cap == r_out - source * cap) & (r_out // cap == source)
    takes = takes.astype(F32).astype(BF16)
    left, told = joined([info_all[s] for s in range(ep)], 1), jnp.zeros((n_rows, tokens), F32)
    for piece in range(3):
        taken = left.astype(BF16)
        told = told + mm(taken, takes)
        left = left - taken.astype(F32)
    ranks = mm(told.astype(BF16), upper)
    for e in range(local):
        where_to = iota((cap_e, tokens), 0).astype(F32) == ranks[e : e + 1]
        placed = jnp.where(where_to, told[e : e + 1], 0.0)
        place_s[e * cap_e : (e + 1) * cap_e, :] = placed.astype(BF16)
        left = jnp.transpose(placed * told[local + e : local + e + 1])
        for piece in range(back_s.shape[0]):
            taken = left.astype(BF16)
            back_s[piece, :, e * cap_e : (e + 1) * cap_e] = taken
            left = left - taken.astype(F32)


    relay(ep - 1)
    for step in range(1, ep):
        s = lax.rem(me + step, ep)
        landed(sc_all.at[s], t_recv.at[s])
    left, row = joined([sc_all[s] for s in range(ep)], 1), jnp.zeros((8, tokens), F32)
    for piece in range(3):
        taken = left.astype(BF16)
        row = row + mm(taken, takes)
        left = left - taken.astype(F32)
    scale = jnp.transpose(jnp.broadcast_to(row[:1], (tokens, tokens)))[:, :1]
    for step in range(1, tp):
        t = lax.rem(mt + step, tp)
        landed(gall.at[t], g_recv.at[t])

    def origin_of(step):
        return lax.rem(chip + step, chips)

    def weights_of(step):
        return pl.ds(pl.multiple_of(origin_of(step) * 2 * dl, 2 * dl), 2 * dl)

    def gained(step):
        for side in range(2):
            t = origin_of(step) * 2 + side
            xw_s[:, side * dl : (side + 1) * dl] = (xall[t].astype(F32) * scale * gall[t]).astype(BF16)

    def mates(step):
        for s in range(ep):
            landed(chunk_of(origin_of(step) * 2 + 1 - core, s), gc_recv.at[origin_of(step), s])

    mates(0)
    gained(0)

    for e in range(local):
        weight(0, e).wait()
        weight(1, e).wait()
    for e in range(local):
        gacc_s[e] = mm(xw_s[...], wg_v[e, weights_of(0), :])
        uacc_s[e] = mm(xw_s[...], wu_v[e, weights_of(0), :])
    outputs()
    for step in range(1, chips - 1):
        mates(step)
        gained(step)
        for e in range(local):
            gacc_s[e] = gacc_s[e] + mm(xw_s[...], wg_v[e, weights_of(step), :])
            uacc_s[e] = uacc_s[e] + mm(xw_s[...], wu_v[e, weights_of(step), :])
    mates(chips - 1)
    gained(chips - 1)

    def sums(e):
        part = weights_of(chips - 1)
        return gacc_s[e] + mm(xw_s[...], wg_v[e, part, :]), uacc_s[e] + mm(xw_s[...], wu_v[e, part, :])

    following = sums(0)
    for e in range(local):
        rows = expert_rows(e)
        gate, up = following
        if e + 1 < local:
            following = sums(e + 1)
        hidden = (gate / (1.0 + jnp.exp(-gate)) * up).astype(BF16)
        hidden = mm(place_s[rows, :], hidden).astype(BF16)
        hmine[rows, :] = hidden
        hall[mt, rows, :] = hidden
        for step in range(1, chips):
            h_over_x(step, e).start()
        h_to_mate(0, e).start()

    pl.when(me == 1)(chain_turn(0, heads))

    def finals():
        for u in range(heads * chunks):
            h, c = u // chunks, u % chunks
            mixed = mm(sc_s[u], twice(sin_s[h])) + y_s[u]
            query = q_s[c * 128 : (c + 1) * 128, h * 128 : (h + 1) * 128].astype(F32)
            squared = jnp.sum(query * query, -1, keepdims=True) + EPSILON
            rq = lax.rsqrt(squared) * (128 ** (-0.5))
            factor = rq * lax.rsqrt(jnp.mean(mixed * mixed, -1, keepdims=True) * (rq * rq) + EPSILON)
            flat_s[pl.ds(c * 128 * heads + h, 128, stride=heads), :] = mixed * factor * ngain_ref[...]
        mix_ref[...] = flat_s[...].astype(BF16)

    @pl.when(me == 0)
    def _():
        sin_s[...] = jnp.zeros_like(sin_s)

    units = 2 * hall.shape[2]

    def hidden_of(step, e):
        rows = expert_rows(e)
        landed(hall.at[origin_of(step) * 2 + 1 - core, rows], hc_recv.at[origin_of(step), e])
        return joined([hall[origin_of(step) * 2 + side, rows, :] for side in range(2)], 1)

    def downs(step, e):
        return wd_v[e, pl.ds(pl.multiple_of(origin_of(step) * units, units), units), :]

    for e in range(local):
        weight(2, e).wait()
    for e in range(local // 2):
        h_relay(e)
    for step in range(chips - 1):
        for e in range(local):
            rows = slice(e * cap_e, (e + 1) * cap_e)
            out = mm(hidden_of(step, e), downs(step, e))
            dacc_s[rows, :] = out if step == 0 else dacc_s[rows, :] + out
    for e in range(local // 2, local):
        h_relay(e)
    pl.when(me == 2)(chain_turn(0, heads))
    for e in range(local):
        rows = slice(e * cap_e, (e + 1) * cap_e)
        out = dacc_s[rows, :] + mm(hidden_of(chips - 1, e), downs(chips - 1, e))
        copies_s[rows, :] = out.astype(BF16)
    own = pl.ds(pl.multiple_of(me * cap, cap), cap)
    for part in range(parts):
        lanes = slice(part * wide_part, (part + 1) * wide_part)
        result = mm(joined([back_s[piece] for piece in range(back_s.shape[0])], 1), twice(copies_s[:, lanes]))
        ret_out[:, lanes] = result.astype(BF16)
        ret_in[own, lanes] = ret_out[own, lanes]
        for step in range(1, ep):
            giving(step, part).start()

    pl.when(me >= 3)(chain_turn(0, heads))
    finals()
    written = (
        pltpu.make_async_copy(mix_ref, mix_hbm, out_sem.at[0]),
        pltpu.make_async_copy(ffn_ref, ffn_hbm, out_sem.at[1]),
    )
    written[0].start()

    for step in range(1, ep):
        s = lax.rem(me + step, ep)
        for part in range(parts):
            lanes = slice(part * wide_part, (part + 1) * wide_part)
            landed(ret_in.at[pl.ds(pl.multiple_of(s * cap, cap), cap), lanes], r_recv.at[s, part])
    ffn_ref[...] = mm(perm_s[...], ret_in[...], COLS_COLS).astype(BF16)
    written[1].start()

    for step in range(1, ep):
        dispatch(step).wait_send()
        scales(step).wait_send()
        tell(step).wait_send()
        for part in range(parts):
            giving(step, part).wait_send()
    for step in range(1, tp):
        gains(step).wait_send()
        squares(step).wait_send()
    for step in range(1, chips):
        for e in range(local):
            h_over_x(step, e).wait_send()
        for s in range(ep):
            over_x(step, s).wait_send()
    for step in range(chips):
        for e in range(local):
            h_to_mate(step, e).wait_send()
        for s in range(ep):
            to_mate(step, s).wait_send()

    @pl.when(me < ep - 1)
    def _():
        def sent(h, carry):
            chain_copy(h).wait_send()
            return carry

        lax.fori_loop(0, heads, sent, 0)

    for copy in written:
        copy.wait()


def hand_on(mix_ref, ffn_ref, mix_out, ffn_out):
    mix_out[...] = mix_ref[...]
    ffn_out[...] = ffn_ref[...]


def fused_body(
    mix_query, mix_keys, mix_values, beta_in, decay_in, norm_gain, ffn_input, ffn_gain,
    expert_ids, expert_share, w_gate, w_up, w_down,
):
    ep, tp = lax.axis_size("ep"), lax.axis_size("tp")
    length, heads, width = mix_query.shape
    tokens, dl = ffn_input.shape
    local, full, fl = w_gate.shape
    out_width = w_down.shape[2]
    picks = expert_ids.shape[1]
    n_rows = max(8, 2 * local)
    chips = tp // 2
    rows_e = tokens * picks
    parts = max(1, min(2, out_width // 512))
    dma = pltpu.SemaphoreType.DMA
    vmem = pl.BlockSpec(memory_space=pltpu.VMEM)
    units = heads * (length // width)
    mix_out, ffn_out = pl.pallas_call(
        layer_kernel,
        out_shape=(
            jax.ShapeDtypeStruct((length * heads, width), BF16),
            jax.ShapeDtypeStruct((tokens, out_width), BF16),
        ),
        in_specs=[pl.BlockSpec(memory_space=pltpu.HBM)] * 13,
        out_specs=(pl.BlockSpec(memory_space=pltpu.HBM),) * 2,
        scratch_shapes=[
            pltpu.VMEM((length * heads, width), BF16),
            pltpu.VMEM((tokens, out_width), BF16),
            dma((2,)),
            pltpu.VMEM((length * heads, width), BF16),
            pltpu.VMEM((length * heads, width), BF16),
            pltpu.VMEM((length * heads, width), BF16),
            pltpu.VMEM(beta_in.shape, F32),
            pltpu.VMEM(decay_in.shape, F32),
            pltpu.VMEM((1, width), F32),
            pltpu.VMEM(ffn_input.shape, BF16),
            pltpu.VMEM((1, dl), F32),
            pltpu.VMEM((picks, tokens), jnp.int32),
            pltpu.VMEM((picks, tokens), F32),
            dma((10,)),
            pltpu.VMEM((length, heads * width), BF16),
            pltpu.VMEM((length, heads * width), BF16),
            pltpu.VMEM((length, heads * width), BF16),
            pltpu.VMEM((length * heads, width), F32),
            pltpu.VMEM((128, 128), F32),
            pltpu.VMEM((128, 128), F32),
            pltpu.VMEM((units, width, 2 * width), BF16),
            pltpu.VMEM((max(units - heads, 1), width, 2 * width), BF16),
            pltpu.VMEM((units, width, width), F32),
            pltpu.VMEM((units, width, width), F32),
            pltpu.VMEM((units, width, width), F32),
            pltpu.VMEM((heads, width, 2 * width), BF16),
            pltpu.VMEM((heads, width, width), F32),
            pltpu.VMEM((heads, width, width), BF16),
            pltpu.VMEM((heads, width, width), BF16),
            pltpu.VMEM(w_gate.shape, BF16),
            pltpu.VMEM(w_up.shape, BF16),
            pltpu.VMEM(w_down.shape, BF16),
            pltpu.VMEM((tokens, tokens), BF16),
            pltpu.VMEM((tokens, dl), BF16),
            pltpu.VMEM((n_rows, tokens), F32),
            pltpu.VMEM((ep, n_rows, tokens), F32),
            pltpu.VMEM((tp, 8, tokens), F32),
            pltpu.VMEM((8, tokens), F32),
            pltpu.VMEM((ep, 8, tokens), F32),
            pltpu.VMEM((tp, 1, dl), F32),
            pltpu.VMEM((tp, tokens, dl), BF16),
            pltpu.VMEM((tokens, full // chips), BF16),
            pltpu.VMEM((local, tokens, fl), F32),
            pltpu.VMEM((local, tokens, fl), F32),
            pltpu.VMEM((rows_e, fl), BF16),
            pltpu.VMEM((tp, rows_e, fl), BF16),
            pltpu.VMEM((rows_e, tokens), BF16),
            pltpu.VMEM((2, tokens, rows_e), BF16),
            pltpu.VMEM((rows_e, out_width), F32),
            pltpu.VMEM((rows_e, out_width), BF16),
            pltpu.VMEM((tokens, out_width), BF16),
            pltpu.VMEM((tokens, out_width), BF16),
            dma((3, local)),
            dma((ep,)), dma((ep,)), dma((ep,)), dma((ep,)),
            dma((tp,)), dma((tp,)), dma((tp,)), dma((tp,)),
            dma((ep,)), dma((ep,)),
            dma((chips, ep)), dma((chips, ep)), dma((chips, ep)), dma((chips, ep)),
            dma((chips, local)), dma((chips, local)), dma((chips, local)), dma((chips, local)),
            dma((ep, parts)), dma((ep, parts)),
            dma((heads,)), dma((heads,)),
        ],
        compiler_params=pltpu.CompilerParams(
            collective_id=0, has_side_effects=True, vmem_limit_bytes=60 * 1024 * 1024
        ),
    )(
        mix_query.reshape(length * heads, width),
        mix_keys.reshape(length * heads, width),
        mix_values.reshape(length * heads, width),
        beta_in, decay_in, norm_gain.reshape(1, width),
        ffn_input, ffn_gain.reshape(1, dl), expert_ids.T, expert_share.T,
        w_gate, w_up, w_down,
    )
    mix_out, ffn_out = pl.pallas_call(
        hand_on,
        out_shape=(
            jax.ShapeDtypeStruct(mix_out.shape, BF16),
            jax.ShapeDtypeStruct(ffn_out.shape, BF16),
        ),
        in_specs=[vmem] * 2,
        out_specs=(vmem, vmem),
        cost_estimate=pl.CostEstimate(flops=1000, bytes_accessed=2**21, transcendentals=0),
    )(mix_out, ffn_out)
    return (mix_out.reshape(length, heads, width), ffn_out)


def body(
    mix_query,
    mix_keys,
    mix_values,
    beta_in,
    decay_in,
    norm_gain,
    ffn_input,
    ffn_gain,
    expert_ids,
    expert_share,
    w_gate,
    w_up,
    w_down,
):
    width, local = mix_query.shape[2], w_gate.shape[0]
    whole_groups = local % GROUP == 0 and expert_ids.shape[1] == 2
    even = lax.axis_size("tp") % 2 == 0 and lax.axis_size("tp") > 1 and lax.axis_size("ep") > 1
    units = mix_query.shape[1] * mix_query.shape[0] // 128
    if whole_groups and even and units % 8 == 0 and units < 25 and width == 128 and mix_query.shape[0] % 128 == 0:
        return fused_body(
            mix_query,
            mix_keys,
            mix_values,
            beta_in,
            decay_in,
            norm_gain,
            ffn_input,
            ffn_gain,
            expert_ids,
            expert_share,
            w_gate,
            w_up,
            w_down,
        )
    mix_out = mixer_body(mix_query, mix_keys, mix_values, beta_in, decay_in, norm_gain)
    ffn_out = experts_body(ffn_input, ffn_gain, expert_ids, expert_share, w_gate, w_up, w_down)
    return (mix_out, ffn_out)


def solution(mesh):
    placed = (
        P(("grp", "ep"), "tp", None),
        P(("grp", "ep"), "tp", None),
        P(("grp", "ep"), "tp", None),
        P("tp", ("grp", "ep")),
        P("tp", ("grp", "ep")),
        P(),
        P(("grp", "ep"), "tp"),
        P("tp"),
        P(("grp", "ep"), None),
        P(("grp", "ep"), None),
        P("ep", None, "tp"),
        P("ep", None, "tp"),
        P("ep", None, "tp"),
    )
    return jax.shard_map(
        body,
        mesh=mesh,
        in_specs=placed,
        out_specs=(P(("grp", "ep"), "tp", None), P(("grp", "ep"), "tp")),
        check_vma=False,
    )
```

```python
import functools
import jax
import jax.numpy as jnp
from jax import lax
from jax.experimental import pallas as pl
from jax.experimental.pallas import tpu as pltpu
from jax.sharding import PartitionSpec as P

BLOCK = 64
GROUP = 4
F32 = jnp.float32
BF16 = jnp.bfloat16
MESH = pl.DeviceIdType.MESH
ROWS_COLS = (((1,), (0,)), ((), ()))
ROWS_ROWS = (((1,), (1,)), ((), ()))
COLS_COLS = (((0,), (0,)), ((), ()))


PRECISE = lax.Precision.HIGHEST
EPSILON = 1e-06


def entering_2(value, axis, join, neutral):
    count, mine = (lax.axis_size(axis), lax.axis_index(axis))
    pieces = jax.tree.map(lambda part: lax.all_gather(part, axis), value)
    subtotal = jax.tree.map(
        lambda part, zero: jnp.full_like(part, 0) + jnp.asarray(zero, part.dtype), value, neutral
    )

    def turn(position, subtotal):
        longer = join(subtotal, jax.tree.map(lambda part: part[position], pieces))
        return jax.tree.map(lambda new, old: jnp.where(position < mine, new, old), longer, subtotal)

    return lax.fori_loop(0, count - 1, turn, subtotal)


def unit_inverse(strict_lower):
    extent = strict_lower.shape[-1]
    identity = jnp.eye(extent, dtype=jnp.float32)
    powered = -strict_lower
    product = identity + powered
    for section_index in range(1, (extent - 1).bit_length()):
        powered = jnp.matmul(powered, powered, precision=PRECISE)
        product = jnp.matmul(product, identity + powered, precision=PRECISE)
    return product


def block_terms(queries, keyset, valueset, betas, rates):
    extent = queries.shape[-2]
    cumulative = -jnp.cumsum(rates, axis=-1)
    positions = jnp.arange(extent)
    causal = positions[:, None] >= positions[None, :]
    strict = positions[:, None] > positions[None, :]
    spread = cumulative[..., :, None] - cumulative[..., None, :]
    decay_mask = jnp.where(causal, jnp.exp(jnp.where(causal, spread, 0.0)), 0.0)
    keys_beta = keyset * betas[..., None]
    values_beta = valueset * betas[..., None]
    lower_part = jnp.where(
        strict,
        jnp.einsum("...id,...jd->...ij", keys_beta, keyset, precision=PRECISE) * decay_mask,
        0.0,
    )
    inverse = unit_inverse(lower_part)
    update = jnp.einsum("...ij,...jd->...id", inverse, values_beta, precision=PRECISE)
    correction = jnp.einsum(
        "...ij,...jd->...id", inverse, keys_beta * jnp.exp(cumulative)[..., None], precision=PRECISE
    )
    scores = jnp.where(
        causal,
        jnp.einsum("...id,...jd->...ij", queries, keyset, precision=PRECISE) * decay_mask,
        0.0,
    )
    query_decay = queries * jnp.exp(cumulative)[..., None]
    key_decay = keyset * jnp.exp(cumulative[..., -1:] - cumulative)[..., None]
    block_decay = jnp.exp(cumulative[..., -1])
    return (query_decay, key_decay, update, correction, scores, block_decay)


def unit_rows(values_in, factor):
    floats = values_in.astype(jnp.float32)
    return floats * lax.rsqrt(jnp.sum(floats * floats, -1, keepdims=True) + EPSILON) * factor


def compose(earlier, later):
    return (
        jnp.matmul(later[0], earlier[0], precision=PRECISE),
        jnp.matmul(later[0], earlier[1], precision=PRECISE) + later[1],
    )


def mixer_body(mix_query, mix_keys, mix_values, beta_in, decay_in, norm_gain):
    length, head_count, width = mix_query.shape
    blocks = length // BLOCK

    def to_blocks(tensor):
        return tensor.reshape(blocks, BLOCK, head_count, width).transpose(2, 0, 1, 3)

    queries = to_blocks(unit_rows(mix_query, width ** (-0.5)))
    keyset = to_blocks(unit_rows(mix_keys, 1.0))
    valueset = to_blocks(mix_values.astype(jnp.float32))
    betas = jax.nn.sigmoid(beta_in).reshape(head_count, blocks, BLOCK)
    rates = jax.nn.softplus(decay_in).reshape(head_count, blocks, BLOCK)
    query_decay, key_decay, update, correction, scores, block_decay = block_terms(
        queries, keyset, valueset, betas, rates
    )
    identity = jnp.eye(width, dtype=jnp.float32)
    transfer = block_decay[..., None, None] * identity - jnp.einsum(
        "hncd,hnce->hnde", key_decay, correction, precision=PRECISE
    )
    offset = jnp.einsum("hncd,hnce->hnde", key_decay, update, precision=PRECISE)
    prefix_map, prefix_add = lax.associative_scan(compose, (transfer, offset), axis=1)
    total_map = prefix_map[:, -1]
    total_add = prefix_add[:, -1]
    empty_state = jnp.zeros((head_count, width, width), jnp.float32)
    unit_maps = jnp.broadcast_to(identity, (head_count, width, width))
    ignored_map, entering = entering_2(
        (total_map, total_add), "ep", compose, (unit_maps, empty_state)
    )
    after_blocks = jnp.matmul(prefix_map, entering[:, None], precision=PRECISE) + prefix_add
    starts = jnp.concatenate([entering[:, None], after_blocks[:, :-1]], axis=1)
    fresh = update - jnp.einsum("hncd,hnde->hnce", correction, starts, precision=PRECISE)
    outputs = jnp.einsum("hncd,hnde->hnce", query_decay, starts, precision=PRECISE) + jnp.einsum(
        "hnij,hnje->hnie", scores, fresh, precision=PRECISE
    )
    raw_mix = outputs.transpose(1, 2, 0, 3).reshape(length, head_count, width)
    return (
        raw_mix * lax.rsqrt(jnp.mean(raw_mix * raw_mix, -1, keepdims=True) + EPSILON) * norm_gain
    ).astype(jnp.bfloat16)


def experts_body(ffn_input, ffn_gain, expert_ids, expert_share, w_gate, w_up, w_down):
    floats = ffn_input.astype(jnp.float32)
    square_sum = lax.psum(jnp.sum(floats * floats, -1), "tp")
    full_width = ffn_input.shape[1] * lax.axis_size("tp")
    normed = (floats * lax.rsqrt(square_sum / full_width + EPSILON)[:, None] * ffn_gain).astype(
        jnp.bfloat16
    )
    pick_count = expert_ids.shape[1]
    flat_ids = expert_ids.reshape(-1)
    sort_order = jnp.argsort(flat_ids, stable=True)
    source_rows = sort_order // pick_count
    experts_local = w_gate.shape[0]
    expert_devices = lax.axis_size("ep")
    capacity = flat_ids.shape[0] // (experts_local * expert_devices)
    outgoing = normed[source_rows].reshape(expert_devices, experts_local, capacity, normed.shape[1])
    arrived = lax.all_to_all(outgoing, "ep", split_axis=0, concat_axis=0, tiled=True)
    slab_in = lax.all_gather(arrived, "tp", axis=3, tiled=True)
    gate_sum = jnp.einsum("secl,elf->secf", slab_in, w_gate, preferred_element_type=jnp.float32)
    up_sum = jnp.einsum("secl,elf->secf", slab_in, w_up, preferred_element_type=jnp.float32)
    hidden = (jax.nn.silu(gate_sum) * up_sum).astype(jnp.bfloat16)
    merged = jnp.einsum(
        "secf,efd->secd",
        lax.all_gather(hidden, "tp", axis=3, tiled=True),
        w_down,
        preferred_element_type=jnp.float32,
    )
    copies = merged.astype(jnp.bfloat16)
    returned = lax.all_to_all(copies, "ep", split_axis=0, concat_axis=0, tiled=True).reshape(
        -1, w_down.shape[2]
    )
    slots = jnp.argsort(sort_order)
    per_slot = returned[slots].reshape(expert_ids.shape[0], pick_count, -1)
    return jnp.sum(per_slot.astype(jnp.float32) * expert_share[..., None], axis=1).astype(
        jnp.bfloat16
    )

def mm(a, b, dims=ROWS_COLS):
    return lax.dot_general(a, b, dims, preferred_element_type=F32)


def exact(a, b, dims=ROWS_COLS):
    return lax.dot_general(a, b, dims, preferred_element_type=F32, precision=PRECISE)


def halves(a):
    high = a.astype(BF16)
    return high, (a - high.astype(F32)).astype(BF16)


def joined(parts, dim):
    return jnp.concatenate(parts, dim)


def split(a):
    return joined(halves(a), 1)


def twice(b):
    return joined([b, b], 0)


def three(a, b):
    n = b.shape[1]
    bh, bl = halves(b)
    rhs = joined([joined([bh, bl], 1), joined([bh, jnp.zeros_like(bl)], 1)], 0)
    out = mm(split(a), rhs)
    return out[:, :n] + out[:, n:]


def iota(shape, dim):
    return lax.broadcasted_iota(jnp.int32, shape, dim)


def unit_tools(heads, chunks, rows_s, cols_s):
    n = 128
    count = heads * chunks

    def block(ref, u):
        i, c = u // chunks, u % chunks
        return ref[c * n : (c + 1) * n, i * n : (i + 1) * n]

    def row_of(kind, u):
        return rows_s[kind * count + u : kind * count + u + 1, :]

    def col_of(kind, u):
        return cols_s[:, kind * count + u : kind * count + u + 1]

    return block, row_of, col_of


CUM, BETA, DECAY, SUMS, ROOT = range(5)


def solve_all(q_ref, k_ref, rows_s, cols_s, qd_s, sc_s, inv_s, service):
    n = 128
    heads, chunks = k_ref.shape[1] // n, k_ref.shape[0] // n
    count = heads * chunks
    row, col = iota((n, n), 0), iota((n, n), 1)
    causal, strict = row >= col, row > col
    same = (row >= n // 2) == (col >= n // 2)
    inside, outside = strict & same, strict & jnp.logical_not(same)
    diagonal = row == col
    eye = diagonal.astype(F32)
    block, row_of, col_of = unit_tools(heads, chunks, rows_s, cols_s)
    everything = range(count)
    cum = rows_s[:count, :]
    rows_s[DECAY * count : (DECAY + 1) * count, :] = jnp.exp(cum)
    based = cum - jnp.log(rows_s[count : 2 * count, :])
    cols_s[...] = jnp.transpose(joined([cum, jnp.zeros((n - count, n), F32)], 0))
    raws = []
    for u in everything:
        k = block(k_ref, u)
        raws.append(mm(joined([k, block(q_ref, u)], 0), k, ROWS_ROWS))
    prods, powers, offs = [], [], []
    for u in everything:
        raw, ccol = raws[u], col_of(CUM, u)
        total = jnp.sum(jnp.where(diagonal, raw[:n], 0.0), 0, keepdims=True) + EPSILON
        rows_s[SUMS * count + u : SUMS * count + u + 1, :] = total
        dm = jnp.exp(ccol - (based[u : u + 1] + jnp.log(total)))
        sc_s[u] = split(jnp.where(causal, raw[n:] * dm, 0.0))
        qd_s[u] = block(q_ref, u).astype(F32) * jnp.exp(ccol)
        minus = -raw[:n] * dm
        neg = jnp.where(inside, minus, 0.0)
        offs.append(jnp.where(outside, minus, 0.0))
        prods.append(eye + neg)
        powers.append(neg)
    service(0)
    powers = [three(p, p) for p in powers]
    for turn in range((BLOCK - 1).bit_length() - 2):
        both = [three(joined([a, p], 0), p) for a, p in zip(prods, powers)]
        prods = [a + b[:n] for a, b in zip(prods, both)]
        powers = [b[n:] for b in both]
    service(1)
    prods = [a + three(a, p) for a, p in zip(prods, powers)]
    mids = [three(o, a) for o, a in zip(offs, prods)]
    for u in everything:
        inv_s[u] = prods[u] + three(prods[u], mids[u])
    service(2)


def advanced(steps, adds, state):
    sh, sl = halves(state)
    th, tl = halves(steps)
    out = mm(joined([th, tl], 1), twice(sh)) + mm(th, sl)
    return out + joined([jnp.zeros_like(adds), adds], 1)


def carry_all(k_ref, v_ref, rows_s, cols_s, inv_s, sc_s, qd_s, y_s, z_s, m_s, n_s):
    n = 128
    heads, chunks = k_ref.shape[1] // n, k_ref.shape[0] // n
    count = heads * chunks
    eye = (iota((n, n), 0) == iota((n, n), 1)).astype(F32)
    block, row_of, col_of = unit_tools(heads, chunks, rows_s, cols_s)
    everything = range(count)
    totals, cum = rows_s[SUMS * count : (SUMS + 1) * count, :], rows_s[:count, :]
    rows_s[ROOT * count : (ROOT + 1) * count, :] = jnp.sqrt(totals)
    tail = rows_s[BETA * count : (BETA + 1) * count, :] / totals * jnp.exp(cum[:, n - 1 :] - cum)
    cols_s[...] = jnp.transpose(joined([tail, jnp.zeros((n - count, n), F32)], 0))
    pairs, steps, states, narrow = [], [], [], []
    for u in everything:
        k, v = block(k_ref, u), block(v_ref, u)
        solved = inv_s[u]
        x, w = solved * row_of(ROOT, u), solved * row_of(DECAY, u)
        pairs.append(joined([mm(split(w), twice(k)), mm(split(x), twice(v))], 1))
    for u in everything:
        narrow.append(pairs[u].astype(BF16))
        sh, sl = halves(pairs[u] * col_of(0, u))
        kt = jnp.transpose(block(k_ref, u).astype(F32)).astype(BF16)
        moved = mm(joined([kt, kt], 1), joined([sh, sl], 0))
        last = jnp.exp(row_of(CUM, u)[:, n - 1 :])
        steps.append((last * eye - moved[:, :n], moved[:, n:]))

    def spread_out(units):
        for u in units:
            spread = mm(sc_s[u], twice(narrow[u]))
            sc_s[u] = split(qd_s[u] - spread[:, :n])
            y_s[u] = spread[:, n:]

    def step_of(i, c):
        return steps[i * chunks + c]

    first = [joined(step_of(i, 0), 1) for i in range(heads)]
    if chunks == 4:
        second = [advanced(*step_of(i, 1), first[i]) for i in range(heads)]
        upper = [advanced(*step_of(i, 3), joined(step_of(i, 2), 1)) for i in range(heads)]
        spread_out(everything)
        third = [advanced(*step_of(i, 2), second[i]) for i in range(heads)]
        last = [advanced(upper[i][:, :n], upper[i][:, n:], second[i]) for i in range(heads)]
        states = [first, second, third, last]
    else:
        spread_out(everything)
        states = [first]
        for c in range(1, chunks):
            states.append([advanced(*step_of(i, c), states[-1][i]) for i in range(heads)])
    for i in range(heads):
        m_s[i] = split(states[-1][i][:, :n])
        n_s[i] = states[-1][i][:, n:]
        for c in range(chunks - 1):
            z_s[i * (chunks - 1) + c] = states[c][i].astype(BF16)


def outputs_all(heads, chunks, sc_s, z_s, y_s):
    n = 128
    for u in range(heads * chunks):
        i, c = u // chunks, u % chunks
        if c > 0:
            both = mm(sc_s[u], twice(z_s[i * (chunks - 1) + c - 1]))
            sc_s[u] = split(both[:, :n])
            y_s[u] = y_s[u] + both[:, n:]


def layer_kernel(
    q_hbm, k_hbm, v_hbm, beta_hbm, decay_hbm, ngain_hbm, x_hbm, gain_hbm, ids_hbm, share_hbm,
    wg_ref, wu_ref, wd_ref, mix_ref, ffn_ref,
    q_ref, k_ref, v_ref, beta_ref, decay_ref, ngain_ref, x_ref, gain_ref, ids_ref, share_ref, in_sem,
    q_s, k_s, v_s, flat_s, rows_s, cols_s, sc_s, z_s, qd_s, inv_s, y_s, m_s, n_s, sin_s, sout_s,
    wg_v, wu_v, wd_v, perm_s, disp, info_out, info_all, sq_all, sc_out, sc_all, gall, xall, xw_s, gacc_s, uacc_s, hmine, hall, place_s, back_s, dacc_s, copies_s,
    ret_out, ret_in,
    w_sem, d_send, d_recv, i_send, i_recv, g_send, g_recv, q_send, q_recv, t_send, t_recv,
    gx_send, gx_recv, gc_send, gc_recv, hx_send, hx_recv, hc_send, hc_recv,
    r_send, r_recv, c_send, c_recv,
):
    ep, tp = lax.axis_size("ep"), lax.axis_size("tp")
    me, mt = lax.axis_index("ep"), lax.axis_index("tp")
    chips = tp // 2
    chip, core = mt // 2, lax.rem(mt, 2)
    mate = chip * 2 + 1 - core
    heads, length = beta_ref.shape
    tokens, dl = x_ref.shape
    local = wg_ref.shape[0]
    cap = tokens // ep
    cap_e = tokens * 2 // local
    parts = r_send.shape[1]
    wide_part = ffn_ref.shape[1] // parts

    def nearest(k):
        left, right = me, ep - 1 - me
        inner = jnp.minimum(left, right)
        both = k < 2 * inner
        far = jnp.where(both, k // 2 + 1, k - inner + 1)
        upward = jnp.where(both, k % 2, jnp.where(right > left, 0, 1)) == 0
        return jnp.where(upward, me + far, me - far)

    def away(axis, count, mine, step):
        return {axis: lax.rem(mine + step, count)}

    def remote(src, dst, ssem, rsem, device):
        return pltpu.make_async_remote_copy(
            src_ref=src, dst_ref=dst, send_sem=ssem, recv_sem=rsem,
            device_id=device, device_id_type=MESH,
        )

    barrier = pltpu.get_barrier_semaphore()
    for step in range(1, ep):
        pl.semaphore_signal(barrier, inc=1, device_id=away("ep", ep, me, step), device_id_type=MESH)
    for step in range(1, tp):
        pl.semaphore_signal(barrier, inc=1, device_id=away("tp", tp, mt, step), device_id_type=MESH)

    def weight(which, e):
        src, dst = ((wg_ref, wg_v), (wu_ref, wu_v), (wd_ref, wd_v))[which]
        return pltpu.make_async_copy(src.at[e], dst.at[e], w_sem.at[which, e])

    arriving = [
        pltpu.make_async_copy(src, dst, in_sem.at[i])
        for i, (src, dst) in enumerate((
            (ids_hbm, ids_ref), (x_hbm, x_ref), (share_hbm, share_ref), (gain_hbm, gain_ref),
            (k_hbm, k_ref), (v_hbm, v_ref), (q_hbm, q_ref),
            (beta_hbm, beta_ref), (decay_hbm, decay_ref), (ngain_hbm, ngain_ref),
        ))
    ]
    for copy in arriving:
        copy.start()
    for copy in arriving[:4]:
        copy.wait()

    ids = ids_ref[...]
    first = ids[0:1]
    group = jnp.zeros_like(first)
    for d in range(1, ep):
        group = group + (first >= d * local).astype(jnp.int32)
    n_rows = info_out.shape[0]
    upper = (iota((tokens, tokens), 0) < iota((tokens, tokens), 1)).astype(F32).astype(BF16)
    g_rows = max(8, ep)
    member = (iota((g_rows, tokens), 0) == group).astype(F32)
    rank = jnp.sum(member * mm(member.astype(BF16), upper), 0, keepdims=True)
    slot = group.astype(F32) * cap + rank
    perm = (iota((tokens, tokens), 0).astype(F32) == slot).astype(F32)
    perm_s[...] = perm.astype(BF16)
    disp[...] = mm(perm.astype(BF16), x_ref[...]).astype(BF16)
    l0, l1 = ids[0:1] - group * local, ids[1:2] - group * local
    shares = share_ref[...]
    line = iota((n_rows, tokens), 0)
    picked = ((line == l0) | (line == l1)).astype(F32)
    shared = jnp.where(
        line - local == l0, shares[0:1], jnp.where(line - local == l1, shares[1:2], 0.0)
    )
    info = exact(jnp.where(line < local, picked, shared), perm, ROWS_ROWS)
    info_out[...] = info
    info_all[me] = info
    gall[mt] = gain_ref[...]
    sorted_rows = disp[...].astype(F32)
    sums = jnp.sum(sorted_rows * sorted_rows, -1, keepdims=True)
    sq_all[mt] = jnp.transpose(jnp.broadcast_to(sums, (tokens, tokens)))[:8]
    xall[mt, pl.ds(pl.multiple_of(me * cap, cap), cap), :] = disp[
        pl.ds(pl.multiple_of(me * cap, cap), cap), :
    ]

    def dispatch(step):
        to = nearest(step - 1)
        return remote(
            disp.at[pl.ds(pl.multiple_of(to * cap, cap), cap)],
            xall.at[mt, pl.ds(pl.multiple_of(me * cap, cap), cap)],
            d_send.at[to], d_recv.at[me], {"ep": to},
        )

    def tell(step):
        to = nearest(step - 1)
        return remote(info_out, info_all.at[me], i_send.at[to], i_recv.at[me], {"ep": to})

    def gains(step):
        to = lax.rem(mt + step, tp)
        return remote(gain_ref, gall.at[mt], g_send.at[to], g_recv.at[mt], {"tp": to})

    def squares(step):
        to = lax.rem(mt + step, tp)
        return remote(sq_all.at[mt], sq_all.at[mt], q_send.at[to], q_recv.at[mt], {"tp": to})

    def scales(step):
        to = nearest(step - 1)
        return remote(sc_out, sc_all.at[me], t_send.at[to], t_recv.at[me], {"ep": to})

    def send_scales():
        total = sq_all[mt]
        for step in range(1, tp):
            t = lax.rem(mt + step, tp)
            landed(sq_all.at[t], q_recv.at[t])
            total = total + sq_all[t]
        row = lax.rsqrt(total / (tp * dl) + EPSILON)
        sc_out[...] = row
        sc_all[me] = row
        for step in range(1, ep):
            scales(step).start()

    def chunk_of(origin, s):
        return xall.at[origin, pl.ds(pl.multiple_of(s * cap, cap), cap)]

    def over_x(step, s):
        to = lax.rem(chip + step, chips)
        part = chunk_of(mt, s)
        return remote(part, part, gx_send.at[to, s], gx_recv.at[chip, s], {"tp": to * 2 + core})

    def to_mate(step, s):
        origin = lax.rem(chip + step, chips)
        part = chunk_of(origin * 2 + core, s)
        return remote(part, part, gc_send.at[origin, s], gc_recv.at[origin, s], {"tp": mate})

    def expert_rows(e):
        return pl.ds(pl.multiple_of(e * cap_e, cap_e), cap_e)

    def h_over_x(step, e):
        to = lax.rem(chip + step, chips)
        return remote(
            hmine.at[expert_rows(e)], hall.at[mt, expert_rows(e)],
            hx_send.at[to, e], hx_recv.at[chip, e], {"tp": to * 2 + core},
        )

    def h_to_mate(step, e):
        origin = lax.rem(chip + step, chips)
        part = hall.at[origin * 2 + core, expert_rows(e)]
        src = hmine.at[expert_rows(e)] if step == 0 else part
        return remote(src, part, hc_send.at[origin, e], hc_recv.at[origin, e], {"tp": mate})

    def h_relay(e):
        for step in range(1, chips):
            origin = lax.rem(chip + step, chips)
            landed(hall.at[origin * 2 + core, expert_rows(e)], hx_recv.at[origin, e])
            h_to_mate(step, e).start()

    def giving(step, part):
        to = nearest(ep - 1 - step)
        lanes = slice(part * wide_part, (part + 1) * wide_part)
        return remote(
            ret_out.at[pl.ds(pl.multiple_of(to * cap, cap), cap), lanes],
            ret_in.at[pl.ds(pl.multiple_of(me * cap, cap), cap), lanes],
            r_send.at[to, part], r_recv.at[me, part], {"ep": to},
        )

    def landed(dst, sem):
        pltpu.make_async_copy(dst, dst, sem).wait()

    for copy in arriving[4:]:
        copy.wait()
    for which in range(3):
        for e in range(local):
            weight(which, e).start()

    pl.semaphore_wait(barrier, ep - 1 + tp - 1)
    for step in range(1, tp):
        squares(step).start()
    for step in range(1, ep):
        dispatch(step).start()
        tell(step).start()
    for step in range(1, tp):
        gains(step).start()

    def forward(j):
        s = nearest(j - 1) if j > 0 else me
        if j > 0:
            landed(chunk_of(mt, s), d_recv.at[s])
        for step in range(1, chips):
            over_x(step, s).start()
        to_mate(0, s).start()

    def relay(j):
        s = nearest(j - 1) if j > 0 else me
        for step in range(1, chips):
            origin = lax.rem(chip + step, chips)
            landed(chunk_of(origin * 2 + core, s), gx_recv.at[origin, s])
            to_mate(step, s).start()

    forward(0)

    for src, dst in ((k_ref, k_s), (v_ref, v_s), (q_ref, q_s)):
        flat_s[...] = src[...].astype(F32)
        for h in range(heads):
            for c in range(length // 128):
                dst[c * 128 : (c + 1) * 128, h * 128 : (h + 1) * 128] = flat_s[
                    pl.ds(c * 128 * heads + h, 128, stride=heads), :
                ].astype(BF16)

    strengths = 1.0 / (1.0 + jnp.exp(-beta_ref[...]))
    raw = decay_ref[...]
    small = jnp.exp(-jnp.abs(raw))
    bigger = 1.0 + small
    diff = bigger - 1.0
    log_term = jnp.where(
        diff == 0.0, small, jnp.log(bigger) * small / jnp.where(diff == 0.0, 1.0, diff)
    )
    rates = jnp.maximum(raw, 0.0) + log_term
    ones_upper = (iota((128, 128), 0) <= iota((128, 128), 1)).astype(F32)
    chunks = length // 128
    rows_s[...] = jnp.zeros_like(rows_s)
    for c in range(chunks):
        here = slice(c * 128, (c + 1) * 128)
        summed = -exact(rates[:, here], ones_upper)
        for h in range(heads):
            u = h * chunks + c
            rows_s[u : u + 1, :] = summed[h : h + 1]
            rows_s[heads * chunks + u : heads * chunks + u + 1, :] = strengths[h : h + 1, here]

    def chain_copy(h):
        return remote(sout_s.at[h], sin_s.at[h], c_send.at[h], c_recv.at[h], {"ep": lax.rem(me + 1, ep)})

    def carry_on():
        carry_all(k_s, v_s, rows_s, cols_s, inv_s, sc_s, qd_s, y_s, z_s, m_s, n_s)

        @pl.when(me == 0)
        def _():
            for h in range(heads):
                sout_s[h] = n_s[h].astype(BF16)
                chain_copy(h).start()

    def chain_turn(low, high):
        def turn(h, carry):
            landed(sin_s.at[h], c_recv.at[h])

            @pl.when(me < ep - 1)
            def _():
                sout_s[h] = (mm(m_s[h], twice(sin_s[h])) + n_s[h]).astype(BF16)
                chain_copy(h).start()

            return carry

        def all_turns():
            lax.fori_loop(low, high, turn, 0)

        return all_turns

    def outputs():
        outputs_all(heads, length // 128, sc_s, z_s, y_s)

    def early(place):
        if place == 1:
            send_scales()
            forward(1)
        elif place == 2:
            for j in range(2, ep):
                forward(j)
            relay(0)

    solve_all(q_s, k_s, rows_s, cols_s, qd_s, sc_s, inv_s, early)
    carry_on()

    for step in range(1, ep):
        s = lax.rem(me + step, ep)
        landed(info_all.at[s], i_recv.at[s])
    r_in, r_out = iota((ep * tokens, tokens), 0), iota((ep * tokens, tokens), 1)
    source = r_in // tokens
    takes = (r_in - source * tokens - me * cap == r_out - source * cap) & (r_out // cap == source)
    takes = takes.astype(F32).astype(BF16)
    left, told = joined([info_all[s] for s in range(ep)], 1), jnp.zeros((n_rows, tokens), F32)
    for piece in range(3):
        taken = left.astype(BF16)
        told = told + mm(taken, takes)
        left = left - taken.astype(F32)
    ranks = mm(told.astype(BF16), upper)
    for e in range(local):
        where_to = iota((cap_e, tokens), 0).astype(F32) == ranks[e : e + 1]
        placed = jnp.where(where_to, told[e : e + 1], 0.0)
        place_s[e * cap_e : (e + 1) * cap_e, :] = placed.astype(BF16)
        left = jnp.transpose(placed * told[local + e : local + e + 1])
        for piece in range(back_s.shape[0]):
            taken = left.astype(BF16)
            back_s[piece, :, e * cap_e : (e + 1) * cap_e] = taken
            left = left - taken.astype(F32)


    outputs()
    for j in range(1, ep):
        relay(j)
    for step in range(1, ep):
        s = lax.rem(me + step, ep)
        landed(sc_all.at[s], t_recv.at[s])
    left, row = joined([sc_all[s] for s in range(ep)], 1), jnp.zeros((8, tokens), F32)
    for piece in range(3):
        taken = left.astype(BF16)
        row = row + mm(taken, takes)
        left = left - taken.astype(F32)
    scale = jnp.transpose(jnp.broadcast_to(row[:1], (tokens, tokens)))[:, :1]
    for step in range(1, tp):
        t = lax.rem(mt + step, tp)
        landed(gall.at[t], g_recv.at[t])

    def origin_of(step):
        return lax.rem(chip + step, chips)

    def weights_of(step):
        return pl.ds(pl.multiple_of(origin_of(step) * 2 * dl, 2 * dl), 2 * dl)

    def gained(step):
        for side in range(2):
            t = origin_of(step) * 2 + side
            xw_s[:, side * dl : (side + 1) * dl] = (xall[t].astype(F32) * scale * gall[t]).astype(BF16)

    def mates(step):
        for s in range(ep):
            landed(chunk_of(origin_of(step) * 2 + 1 - core, s), gc_recv.at[origin_of(step), s])

    mates(0)
    gained(0)

    for e in range(local):
        weight(0, e).wait()
        weight(1, e).wait()
    for e in range(local):
        gacc_s[e] = mm(xw_s[...], wg_v[e, weights_of(0), :])
        uacc_s[e] = mm(xw_s[...], wu_v[e, weights_of(0), :])
    for step in range(1, chips - 1):
        mates(step)
        gained(step)
        for e in range(local):
            gacc_s[e] = gacc_s[e] + mm(xw_s[...], wg_v[e, weights_of(step), :])
            uacc_s[e] = uacc_s[e] + mm(xw_s[...], wu_v[e, weights_of(step), :])
    mates(chips - 1)
    gained(chips - 1)

    def sums(e):
        part = weights_of(chips - 1)
        return gacc_s[e] + mm(xw_s[...], wg_v[e, part, :]), uacc_s[e] + mm(xw_s[...], wu_v[e, part, :])

    following = sums(0)
    for e in range(local):
        rows = expert_rows(e)
        gate, up = following
        if e + 1 < local:
            following = sums(e + 1)
        hidden = (gate / (1.0 + jnp.exp(-gate)) * up).astype(BF16)
        hidden = mm(place_s[rows, :], hidden).astype(BF16)
        hmine[rows, :] = hidden
        hall[mt, rows, :] = hidden
        for step in range(1, chips):
            h_over_x(step, e).start()
        h_to_mate(0, e).start()

    pl.when(me == 1)(chain_turn(0, heads))

    def finals():
        for u in range(heads * chunks):
            h, c = u // chunks, u % chunks
            mixed = mm(sc_s[u], twice(sin_s[h])) + y_s[u]
            query = q_s[c * 128 : (c + 1) * 128, h * 128 : (h + 1) * 128].astype(F32)
            squared = jnp.sum(query * query, -1, keepdims=True) + EPSILON
            rq = lax.rsqrt(squared) * (128 ** (-0.5))
            factor = rq * lax.rsqrt(jnp.mean(mixed * mixed, -1, keepdims=True) * (rq * rq) + EPSILON)
            flat_s[pl.ds(c * 128 * heads + h, 128, stride=heads), :] = mixed * factor * ngain_ref[...]
        mix_ref[...] = flat_s[...].astype(BF16)

    @pl.when(me == 0)
    def _():
        sin_s[...] = jnp.zeros_like(sin_s)

    units = 2 * hall.shape[2]

    def hidden_of(step, e):
        rows = expert_rows(e)
        landed(hall.at[origin_of(step) * 2 + 1 - core, rows], hc_recv.at[origin_of(step), e])
        return joined([hall[origin_of(step) * 2 + side, rows, :] for side in range(2)], 1)

    def downs(step, e):
        return wd_v[e, pl.ds(pl.multiple_of(origin_of(step) * units, units), units), :]

    for e in range(local):
        weight(2, e).wait()
    for step in range(chips - 1):
        for e in range(local):
            rows = slice(e * cap_e, (e + 1) * cap_e)
            out = mm(hidden_of(step, e), downs(step, e))
            dacc_s[rows, :] = out if step == 0 else dacc_s[rows, :] + out
    for e in range(local):
        h_relay(e)
    pl.when(me == 2)(chain_turn(0, heads))
    for e in range(local):
        rows = slice(e * cap_e, (e + 1) * cap_e)
        out = dacc_s[rows, :] + mm(hidden_of(chips - 1, e), downs(chips - 1, e))
        copies_s[rows, :] = out.astype(BF16)
    own = pl.ds(pl.multiple_of(me * cap, cap), cap)
    for part in range(parts):
        lanes = slice(part * wide_part, (part + 1) * wide_part)
        result = mm(joined([back_s[piece] for piece in range(back_s.shape[0])], 1), twice(copies_s[:, lanes]))
        ret_out[:, lanes] = result.astype(BF16)
        ret_in[own, lanes] = ret_out[own, lanes]
        for step in range(1, ep):
            giving(step, part).start()

    pl.when(me >= 3)(chain_turn(0, heads))
    finals()
    for step in range(1, ep):
        s = lax.rem(me + step, ep)
        for part in range(parts):
            lanes = slice(part * wide_part, (part + 1) * wide_part)
            landed(ret_in.at[pl.ds(pl.multiple_of(s * cap, cap), cap), lanes], r_recv.at[s, part])
    ffn_ref[...] = mm(perm_s[...], ret_in[...], COLS_COLS).astype(BF16)

    for step in range(1, ep):
        dispatch(step).wait_send()
        scales(step).wait_send()
        tell(step).wait_send()
        for part in range(parts):
            giving(step, part).wait_send()
    for step in range(1, tp):
        gains(step).wait_send()
        squares(step).wait_send()
    for step in range(1, chips):
        for e in range(local):
            h_over_x(step, e).wait_send()
        for s in range(ep):
            over_x(step, s).wait_send()
    for step in range(chips):
        for e in range(local):
            h_to_mate(step, e).wait_send()
        for s in range(ep):
            to_mate(step, s).wait_send()

    @pl.when(me < ep - 1)
    def _():
        def sent(h, carry):
            chain_copy(h).wait_send()
            return carry

        lax.fori_loop(0, heads, sent, 0)


def hand_on(mix_ref, ffn_ref, mix_out, ffn_out, sems):
    copies = [
        pltpu.make_async_copy(mix_ref, mix_out, sems.at[0]),
        pltpu.make_async_copy(ffn_ref, ffn_out, sems.at[1]),
    ]
    for copy in copies:
        copy.start()
    for copy in copies:
        copy.wait()


def fused_body(
    mix_query, mix_keys, mix_values, beta_in, decay_in, norm_gain, ffn_input, ffn_gain,
    expert_ids, expert_share, w_gate, w_up, w_down,
):
    ep, tp = lax.axis_size("ep"), lax.axis_size("tp")
    length, heads, width = mix_query.shape
    tokens, dl = ffn_input.shape
    local, full, fl = w_gate.shape
    out_width = w_down.shape[2]
    picks = expert_ids.shape[1]
    n_rows = max(8, 2 * local)
    chips = tp // 2
    rows_e = tokens * picks
    parts = max(1, min(2, out_width // 512))
    dma = pltpu.SemaphoreType.DMA
    vmem = pl.BlockSpec(memory_space=pltpu.VMEM)
    units = heads * (length // width)
    mix_out, ffn_out = pl.pallas_call(
        layer_kernel,
        out_shape=(
            pltpu.VMEM((length * heads, width), BF16),
            pltpu.VMEM((tokens, out_width), BF16),
        ),
        in_specs=[pl.BlockSpec(memory_space=pltpu.HBM)] * 13,
        out_specs=(vmem, vmem),
        scratch_shapes=[
            pltpu.VMEM((length * heads, width), BF16),
            pltpu.VMEM((length * heads, width), BF16),
            pltpu.VMEM((length * heads, width), BF16),
            pltpu.VMEM(beta_in.shape, F32),
            pltpu.VMEM(decay_in.shape, F32),
            pltpu.VMEM((1, width), F32),
            pltpu.VMEM(ffn_input.shape, BF16),
            pltpu.VMEM((1, dl), F32),
            pltpu.VMEM((picks, tokens), jnp.int32),
            pltpu.VMEM((picks, tokens), F32),
            dma((10,)),
            pltpu.VMEM((length, heads * width), BF16),
            pltpu.VMEM((length, heads * width), BF16),
            pltpu.VMEM((length, heads * width), BF16),
            pltpu.VMEM((length * heads, width), F32),
            pltpu.VMEM((128, 128), F32),
            pltpu.VMEM((128, 128), F32),
            pltpu.VMEM((units, width, 2 * width), BF16),
            pltpu.VMEM((max(units - heads, 1), width, 2 * width), BF16),
            pltpu.VMEM((units, width, width), F32),
            pltpu.VMEM((units, width, width), F32),
            pltpu.VMEM((units, width, width), F32),
            pltpu.VMEM((heads, width, 2 * width), BF16),
            pltpu.VMEM((heads, width, width), F32),
            pltpu.VMEM((heads, width, width), BF16),
            pltpu.VMEM((heads, width, width), BF16),
            pltpu.VMEM(w_gate.shape, BF16),
            pltpu.VMEM(w_up.shape, BF16),
            pltpu.VMEM(w_down.shape, BF16),
            pltpu.VMEM((tokens, tokens), BF16),
            pltpu.VMEM((tokens, dl), BF16),
            pltpu.VMEM((n_rows, tokens), F32),
            pltpu.VMEM((ep, n_rows, tokens), F32),
            pltpu.VMEM((tp, 8, tokens), F32),
            pltpu.VMEM((8, tokens), F32),
            pltpu.VMEM((ep, 8, tokens), F32),
            pltpu.VMEM((tp, 1, dl), F32),
            pltpu.VMEM((tp, tokens, dl), BF16),
            pltpu.VMEM((tokens, full // chips), BF16),
            pltpu.VMEM((local, tokens, fl), F32),
            pltpu.VMEM((local, tokens, fl), F32),
            pltpu.VMEM((rows_e, fl), BF16),
            pltpu.VMEM((tp, rows_e, fl), BF16),
            pltpu.VMEM((rows_e, tokens), BF16),
            pltpu.VMEM((2, tokens, rows_e), BF16),
            pltpu.VMEM((rows_e, out_width), F32),
            pltpu.VMEM((rows_e, out_width), BF16),
            pltpu.VMEM((tokens, out_width), BF16),
            pltpu.VMEM((tokens, out_width), BF16),
            dma((3, local)),
            dma((ep,)), dma((ep,)), dma((ep,)), dma((ep,)),
            dma((tp,)), dma((tp,)), dma((tp,)), dma((tp,)),
            dma((ep,)), dma((ep,)),
            dma((chips, ep)), dma((chips, ep)), dma((chips, ep)), dma((chips, ep)),
            dma((chips, local)), dma((chips, local)), dma((chips, local)), dma((chips, local)),
            dma((ep, parts)), dma((ep, parts)),
            dma((heads,)), dma((heads,)),
        ],
        compiler_params=pltpu.CompilerParams(
            collective_id=0, has_side_effects=True, vmem_limit_bytes=60 * 1024 * 1024
        ),
    )(
        mix_query.reshape(length * heads, width),
        mix_keys.reshape(length * heads, width),
        mix_values.reshape(length * heads, width),
        beta_in, decay_in, norm_gain.reshape(1, width),
        ffn_input, ffn_gain.reshape(1, dl), expert_ids.T, expert_share.T,
        w_gate, w_up, w_down,
    )
    mix_out, ffn_out = pl.pallas_call(
        hand_on,
        out_shape=(
            jax.ShapeDtypeStruct(mix_out.shape, BF16),
            jax.ShapeDtypeStruct(ffn_out.shape, BF16),
        ),
        in_specs=[vmem] * 2,
        out_specs=(pl.BlockSpec(memory_space=pltpu.HBM),) * 2,
        scratch_shapes=[dma((2,))],
        cost_estimate=pl.CostEstimate(flops=1000, bytes_accessed=2**21, transcendentals=0),
        compiler_params=pltpu.CompilerParams(vmem_limit_bytes=4 * 1024 * 1024),
    )(mix_out, ffn_out)
    return (mix_out.reshape(length, heads, width), ffn_out)


def body(
    mix_query,
    mix_keys,
    mix_values,
    beta_in,
    decay_in,
    norm_gain,
    ffn_input,
    ffn_gain,
    expert_ids,
    expert_share,
    w_gate,
    w_up,
    w_down,
):
    width, local = mix_query.shape[2], w_gate.shape[0]
    whole_groups = local % GROUP == 0 and expert_ids.shape[1] == 2
    even = lax.axis_size("tp") % 2 == 0 and lax.axis_size("tp") > 1 and lax.axis_size("ep") > 1
    units = mix_query.shape[1] * mix_query.shape[0] // 128
    if whole_groups and even and units % 8 == 0 and units < 25 and width == 128 and mix_query.shape[0] % 128 == 0:
        return fused_body(
            mix_query,
            mix_keys,
            mix_values,
            beta_in,
            decay_in,
            norm_gain,
            ffn_input,
            ffn_gain,
            expert_ids,
            expert_share,
            w_gate,
            w_up,
            w_down,
        )
    mix_out = mixer_body(mix_query, mix_keys, mix_values, beta_in, decay_in, norm_gain)
    ffn_out = experts_body(ffn_input, ffn_gain, expert_ids, expert_share, w_gate, w_up, w_down)
    return (mix_out, ffn_out)


def solution(mesh):
    placed = (
        P(("grp", "ep"), "tp", None),
        P(("grp", "ep"), "tp", None),
        P(("grp", "ep"), "tp", None),
        P("tp", ("grp", "ep")),
        P("tp", ("grp", "ep")),
        P(),
        P(("grp", "ep"), "tp"),
        P("tp"),
        P(("grp", "ep"), None),
        P(("grp", "ep"), None),
        P("ep", None, "tp"),
        P("ep", None, "tp"),
        P("ep", None, "tp"),
    )
    return jax.shard_map(
        body,
        mesh=mesh,
        in_specs=placed,
        out_specs=(P(("grp", "ep"), "tp", None), P(("grp", "ep"), "tp")),
        check_vma=False,
    )
```

```python
import functools
import jax
import jax.numpy as jnp
from jax import lax
from jax.experimental import pallas as pl
from jax.experimental.pallas import tpu as pltpu
from jax.sharding import PartitionSpec as P

BLOCK = 64
GROUP = 4
F32 = jnp.float32
BF16 = jnp.bfloat16
MESH = pl.DeviceIdType.MESH
ROWS_COLS = (((1,), (0,)), ((), ()))
ROWS_ROWS = (((1,), (1,)), ((), ()))
COLS_COLS = (((0,), (0,)), ((), ()))


PRECISE = lax.Precision.HIGHEST
EPSILON = 1e-06


def entering_2(value, axis, join, neutral):
    count, mine = (lax.axis_size(axis), lax.axis_index(axis))
    pieces = jax.tree.map(lambda part: lax.all_gather(part, axis), value)
    subtotal = jax.tree.map(
        lambda part, zero: jnp.full_like(part, 0) + jnp.asarray(zero, part.dtype), value, neutral
    )

    def turn(position, subtotal):
        longer = join(subtotal, jax.tree.map(lambda part: part[position], pieces))
        return jax.tree.map(lambda new, old: jnp.where(position < mine, new, old), longer, subtotal)

    return lax.fori_loop(0, count - 1, turn, subtotal)


def unit_inverse(strict_lower):
    extent = strict_lower.shape[-1]
    identity = jnp.eye(extent, dtype=jnp.float32)
    powered = -strict_lower
    product = identity + powered
    for section_index in range(1, (extent - 1).bit_length()):
        powered = jnp.matmul(powered, powered, precision=PRECISE)
        product = jnp.matmul(product, identity + powered, precision=PRECISE)
    return product


def block_terms(queries, keyset, valueset, betas, rates):
    extent = queries.shape[-2]
    cumulative = -jnp.cumsum(rates, axis=-1)
    positions = jnp.arange(extent)
    causal = positions[:, None] >= positions[None, :]
    strict = positions[:, None] > positions[None, :]
    spread = cumulative[..., :, None] - cumulative[..., None, :]
    decay_mask = jnp.where(causal, jnp.exp(jnp.where(causal, spread, 0.0)), 0.0)
    keys_beta = keyset * betas[..., None]
    values_beta = valueset * betas[..., None]
    lower_part = jnp.where(
        strict,
        jnp.einsum("...id,...jd->...ij", keys_beta, keyset, precision=PRECISE) * decay_mask,
        0.0,
    )
    inverse = unit_inverse(lower_part)
    update = jnp.einsum("...ij,...jd->...id", inverse, values_beta, precision=PRECISE)
    correction = jnp.einsum(
        "...ij,...jd->...id", inverse, keys_beta * jnp.exp(cumulative)[..., None], precision=PRECISE
    )
    scores = jnp.where(
        causal,
        jnp.einsum("...id,...jd->...ij", queries, keyset, precision=PRECISE) * decay_mask,
        0.0,
    )
    query_decay = queries * jnp.exp(cumulative)[..., None]
    key_decay = keyset * jnp.exp(cumulative[..., -1:] - cumulative)[..., None]
    block_decay = jnp.exp(cumulative[..., -1])
    return (query_decay, key_decay, update, correction, scores, block_decay)


def unit_rows(values_in, factor):
    floats = values_in.astype(jnp.float32)
    return floats * lax.rsqrt(jnp.sum(floats * floats, -1, keepdims=True) + EPSILON) * factor


def compose(earlier, later):
    return (
        jnp.matmul(later[0], earlier[0], precision=PRECISE),
        jnp.matmul(later[0], earlier[1], precision=PRECISE) + later[1],
    )


def mixer_body(mix_query, mix_keys, mix_values, beta_in, decay_in, norm_gain):
    length, head_count, width = mix_query.shape
    blocks = length // BLOCK

    def to_blocks(tensor):
        return tensor.reshape(blocks, BLOCK, head_count, width).transpose(2, 0, 1, 3)

    queries = to_blocks(unit_rows(mix_query, width ** (-0.5)))
    keyset = to_blocks(unit_rows(mix_keys, 1.0))
    valueset = to_blocks(mix_values.astype(jnp.float32))
    betas = jax.nn.sigmoid(beta_in).reshape(head_count, blocks, BLOCK)
    rates = jax.nn.softplus(decay_in).reshape(head_count, blocks, BLOCK)
    query_decay, key_decay, update, correction, scores, block_decay = block_terms(
        queries, keyset, valueset, betas, rates
    )
    identity = jnp.eye(width, dtype=jnp.float32)
    transfer = block_decay[..., None, None] * identity - jnp.einsum(
        "hncd,hnce->hnde", key_decay, correction, precision=PRECISE
    )
    offset = jnp.einsum("hncd,hnce->hnde", key_decay, update, precision=PRECISE)
    prefix_map, prefix_add = lax.associative_scan(compose, (transfer, offset), axis=1)
    total_map = prefix_map[:, -1]
    total_add = prefix_add[:, -1]
    empty_state = jnp.zeros((head_count, width, width), jnp.float32)
    unit_maps = jnp.broadcast_to(identity, (head_count, width, width))
    ignored_map, entering = entering_2(
        (total_map, total_add), "ep", compose, (unit_maps, empty_state)
    )
    after_blocks = jnp.matmul(prefix_map, entering[:, None], precision=PRECISE) + prefix_add
    starts = jnp.concatenate([entering[:, None], after_blocks[:, :-1]], axis=1)
    fresh = update - jnp.einsum("hncd,hnde->hnce", correction, starts, precision=PRECISE)
    outputs = jnp.einsum("hncd,hnde->hnce", query_decay, starts, precision=PRECISE) + jnp.einsum(
        "hnij,hnje->hnie", scores, fresh, precision=PRECISE
    )
    raw_mix = outputs.transpose(1, 2, 0, 3).reshape(length, head_count, width)
    return (
        raw_mix * lax.rsqrt(jnp.mean(raw_mix * raw_mix, -1, keepdims=True) + EPSILON) * norm_gain
    ).astype(jnp.bfloat16)


def experts_body(ffn_input, ffn_gain, expert_ids, expert_share, w_gate, w_up, w_down):
    floats = ffn_input.astype(jnp.float32)
    square_sum = lax.psum(jnp.sum(floats * floats, -1), "tp")
    full_width = ffn_input.shape[1] * lax.axis_size("tp")
    normed = (floats * lax.rsqrt(square_sum / full_width + EPSILON)[:, None] * ffn_gain).astype(
        jnp.bfloat16
    )
    pick_count = expert_ids.shape[1]
    flat_ids = expert_ids.reshape(-1)
    sort_order = jnp.argsort(flat_ids, stable=True)
    source_rows = sort_order // pick_count
    experts_local = w_gate.shape[0]
    expert_devices = lax.axis_size("ep")
    capacity = flat_ids.shape[0] // (experts_local * expert_devices)
    outgoing = normed[source_rows].reshape(expert_devices, experts_local, capacity, normed.shape[1])
    arrived = lax.all_to_all(outgoing, "ep", split_axis=0, concat_axis=0, tiled=True)
    slab_in = lax.all_gather(arrived, "tp", axis=3, tiled=True)
    gate_sum = jnp.einsum("secl,elf->secf", slab_in, w_gate, preferred_element_type=jnp.float32)
    up_sum = jnp.einsum("secl,elf->secf", slab_in, w_up, preferred_element_type=jnp.float32)
    hidden = (jax.nn.silu(gate_sum) * up_sum).astype(jnp.bfloat16)
    merged = jnp.einsum(
        "secf,efd->secd",
        lax.all_gather(hidden, "tp", axis=3, tiled=True),
        w_down,
        preferred_element_type=jnp.float32,
    )
    copies = merged.astype(jnp.bfloat16)
    returned = lax.all_to_all(copies, "ep", split_axis=0, concat_axis=0, tiled=True).reshape(
        -1, w_down.shape[2]
    )
    slots = jnp.argsort(sort_order)
    per_slot = returned[slots].reshape(expert_ids.shape[0], pick_count, -1)
    return jnp.sum(per_slot.astype(jnp.float32) * expert_share[..., None], axis=1).astype(
        jnp.bfloat16
    )

def mm(a, b, dims=ROWS_COLS):
    return lax.dot_general(a, b, dims, preferred_element_type=F32)


def exact(a, b, dims=ROWS_COLS):
    return lax.dot_general(a, b, dims, preferred_element_type=F32, precision=PRECISE)


def halves(a):
    high = a.astype(BF16)
    return high, (a - high.astype(F32)).astype(BF16)


def joined(parts, dim):
    return jnp.concatenate(parts, dim)


def split(a):
    return joined(halves(a), 1)


def twice(b):
    return joined([b, b], 0)


def three(a, b):
    n = b.shape[1]
    bh, bl = halves(b)
    rhs = joined([joined([bh, bl], 1), joined([bh, jnp.zeros_like(bl)], 1)], 0)
    out = mm(split(a), rhs)
    return out[:, :n] + out[:, n:]


def iota(shape, dim):
    return lax.broadcasted_iota(jnp.int32, shape, dim)


def unit_tools(heads, chunks, rows_s, cols_s):
    n = 128
    count = heads * chunks

    def block(ref, u):
        i, c = u // chunks, u % chunks
        return ref[c * n : (c + 1) * n, i * n : (i + 1) * n]

    def row_of(kind, u):
        return rows_s[kind * count + u : kind * count + u + 1, :]

    def col_of(kind, u):
        return cols_s[:, kind * count + u : kind * count + u + 1]

    return block, row_of, col_of


CUM, BETA, DECAY, SUMS, ROOT = range(5)


def solve_all(q_ref, k_ref, rows_s, cols_s, qd_s, sc_s, inv_s, service):
    n = 128
    heads, chunks = k_ref.shape[1] // n, k_ref.shape[0] // n
    count = heads * chunks
    row, col = iota((n, n), 0), iota((n, n), 1)
    causal, strict = row >= col, row > col
    same = (row >= n // 2) == (col >= n // 2)
    inside, outside = strict & same, strict & jnp.logical_not(same)
    diagonal = row == col
    eye = diagonal.astype(F32)
    block, row_of, col_of = unit_tools(heads, chunks, rows_s, cols_s)
    everything = range(count)
    cum = rows_s[:count, :]
    rows_s[DECAY * count : (DECAY + 1) * count, :] = jnp.exp(cum)
    based = cum - jnp.log(rows_s[count : 2 * count, :])
    cols_s[...] = jnp.transpose(joined([cum, jnp.zeros((n - count, n), F32)], 0))
    raws = []
    for u in everything:
        k = block(k_ref, u)
        raws.append(mm(joined([k, block(q_ref, u)], 0), k, ROWS_ROWS))
    prods, powers, offs = [], [], []
    for u in everything:
        raw, ccol = raws[u], col_of(CUM, u)
        total = jnp.sum(jnp.where(diagonal, raw[:n], 0.0), 0, keepdims=True) + EPSILON
        rows_s[SUMS * count + u : SUMS * count + u + 1, :] = total
        dm = jnp.exp(ccol - (based[u : u + 1] + jnp.log(total)))
        sc_s[u] = split(jnp.where(causal, raw[n:] * dm, 0.0))
        qd_s[u] = block(q_ref, u).astype(F32) * jnp.exp(ccol)
        minus = -raw[:n] * dm
        neg = jnp.where(inside, minus, 0.0)
        offs.append(jnp.where(outside, minus, 0.0))
        prods.append(eye + neg)
        powers.append(neg)
    service(0)
    powers = [three(p, p) for p in powers]
    for turn in range((BLOCK - 1).bit_length() - 2):
        both = [three(joined([a, p], 0), p) for a, p in zip(prods, powers)]
        prods = [a + b[:n] for a, b in zip(prods, both)]
        powers = [b[n:] for b in both]
    service(1)
    prods = [a + three(a, p) for a, p in zip(prods, powers)]
    mids = [three(o, a) for o, a in zip(offs, prods)]
    for u in everything:
        inv_s[u] = prods[u] + three(prods[u], mids[u])
    service(2)


def advanced(steps, adds, state):
    sh, sl = halves(state)
    th, tl = halves(steps)
    out = mm(joined([th, tl], 1), twice(sh)) + mm(th, sl)
    return out + joined([jnp.zeros_like(adds), adds], 1)


def carry_all(k_ref, v_ref, rows_s, cols_s, inv_s, sc_s, qd_s, y_s, z_s, m_s, n_s):
    n = 128
    heads, chunks = k_ref.shape[1] // n, k_ref.shape[0] // n
    count = heads * chunks
    eye = (iota((n, n), 0) == iota((n, n), 1)).astype(F32)
    block, row_of, col_of = unit_tools(heads, chunks, rows_s, cols_s)
    everything = range(count)
    totals, cum = rows_s[SUMS * count : (SUMS + 1) * count, :], rows_s[:count, :]
    rows_s[ROOT * count : (ROOT + 1) * count, :] = jnp.sqrt(totals)
    tail = rows_s[BETA * count : (BETA + 1) * count, :] / totals * jnp.exp(cum[:, n - 1 :] - cum)
    cols_s[...] = jnp.transpose(joined([tail, jnp.zeros((n - count, n), F32)], 0))
    pairs, steps, states, narrow = [], [], [], []
    for u in everything:
        k, v = block(k_ref, u), block(v_ref, u)
        solved = inv_s[u]
        x, w = solved * row_of(ROOT, u), solved * row_of(DECAY, u)
        pairs.append(joined([mm(split(w), twice(k)), mm(split(x), twice(v))], 1))
    for u in everything:
        narrow.append(pairs[u].astype(BF16))
        sh, sl = halves(pairs[u] * col_of(0, u))
        kt = jnp.transpose(block(k_ref, u).astype(F32)).astype(BF16)
        moved = mm(joined([kt, kt], 1), joined([sh, sl], 0))
        last = jnp.exp(row_of(CUM, u)[:, n - 1 :])
        steps.append((last * eye - moved[:, :n], moved[:, n:]))

    def spread_out(units):
        for u in units:
            spread = mm(sc_s[u], twice(narrow[u]))
            sc_s[u] = split(qd_s[u] - spread[:, :n])
            y_s[u] = spread[:, n:]

    def step_of(i, c):
        return steps[i * chunks + c]

    first = [joined(step_of(i, 0), 1) for i in range(heads)]
    if chunks == 4:
        second = [advanced(*step_of(i, 1), first[i]) for i in range(heads)]
        upper = [advanced(*step_of(i, 3), joined(step_of(i, 2), 1)) for i in range(heads)]
        spread_out(everything)
        third = [advanced(*step_of(i, 2), second[i]) for i in range(heads)]
        last = [advanced(upper[i][:, :n], upper[i][:, n:], second[i]) for i in range(heads)]
        states = [first, second, third, last]
    else:
        spread_out(everything)
        states = [first]
        for c in range(1, chunks):
            states.append([advanced(*step_of(i, c), states[-1][i]) for i in range(heads)])
    for i in range(heads):
        m_s[i] = split(states[-1][i][:, :n])
        n_s[i] = states[-1][i][:, n:]
        for c in range(chunks - 1):
            z_s[i * (chunks - 1) + c] = states[c][i].astype(BF16)


def outputs_all(heads, chunks, sc_s, z_s, y_s):
    n = 128
    for u in range(heads * chunks):
        i, c = u // chunks, u % chunks
        if c > 0:
            both = mm(sc_s[u], twice(z_s[i * (chunks - 1) + c - 1]))
            sc_s[u] = split(both[:, :n])
            y_s[u] = y_s[u] + both[:, n:]


def layer_kernel(
    q_hbm, k_hbm, v_hbm, beta_hbm, decay_hbm, ngain_hbm, x_hbm, gain_hbm, ids_hbm, share_hbm,
    wg_ref, wu_ref, wd_ref, mix_ref, ffn_ref,
    q_ref, k_ref, v_ref, beta_ref, decay_ref, ngain_ref, x_ref, gain_ref, ids_ref, share_ref, in_sem,
    q_s, k_s, v_s, flat_s, rows_s, cols_s, sc_s, z_s, qd_s, inv_s, y_s, m_s, n_s, sin_s, sout_s,
    wg_v, wu_v, wd_v, perm_s, disp, info_out, info_all, sq_all, sc_out, sc_all, gall, xall, xw_s, gacc_s, uacc_s, hmine, hall, place_s, back_s, dacc_s, copies_s,
    ret_out, ret_in,
    w_sem, d_send, d_recv, i_send, i_recv, g_send, g_recv, q_send, q_recv, t_send, t_recv,
    gx_send, gx_recv, gc_send, gc_recv, hx_send, hx_recv, hc_send, hc_recv,
    r_send, r_recv, c_send, c_recv,
):
    ep, tp = lax.axis_size("ep"), lax.axis_size("tp")
    me, mt = lax.axis_index("ep"), lax.axis_index("tp")
    chips = tp // 2
    chip, core = mt // 2, lax.rem(mt, 2)
    mate = chip * 2 + 1 - core
    heads, length = beta_ref.shape
    tokens, dl = x_ref.shape
    local = wg_ref.shape[0]
    cap = tokens // ep
    cap_e = tokens * 2 // local
    parts = r_send.shape[1]
    wide_part = ffn_ref.shape[1] // parts

    def nearest(k):
        left, right = me, ep - 1 - me
        inner = jnp.minimum(left, right)
        both = k < 2 * inner
        far = jnp.where(both, k // 2 + 1, k - inner + 1)
        upward = jnp.where(both, k % 2, jnp.where(right > left, 0, 1)) == 0
        return jnp.where(upward, me + far, me - far)

    def away(axis, count, mine, step):
        return {axis: lax.rem(mine + step, count)}

    def remote(src, dst, ssem, rsem, device):
        return pltpu.make_async_remote_copy(
            src_ref=src, dst_ref=dst, send_sem=ssem, recv_sem=rsem,
            device_id=device, device_id_type=MESH,
        )

    barrier = pltpu.get_barrier_semaphore()
    for step in range(1, ep):
        pl.semaphore_signal(barrier, inc=1, device_id=away("ep", ep, me, step), device_id_type=MESH)
    for step in range(1, tp):
        pl.semaphore_signal(barrier, inc=1, device_id=away("tp", tp, mt, step), device_id_type=MESH)

    def weight(which, e):
        src, dst = ((wg_ref, wg_v), (wu_ref, wu_v), (wd_ref, wd_v))[which]
        return pltpu.make_async_copy(src.at[e], dst.at[e], w_sem.at[which, e])

    arriving = [
        pltpu.make_async_copy(src, dst, in_sem.at[i])
        for i, (src, dst) in enumerate((
            (ids_hbm, ids_ref), (x_hbm, x_ref), (share_hbm, share_ref), (gain_hbm, gain_ref),
            (k_hbm, k_ref), (v_hbm, v_ref), (q_hbm, q_ref),
            (beta_hbm, beta_ref), (decay_hbm, decay_ref), (ngain_hbm, ngain_ref),
        ))
    ]
    for copy in arriving:
        copy.start()
    for copy in arriving[:4]:
        copy.wait()

    ids = ids_ref[...]
    first = ids[0:1]
    group = jnp.zeros_like(first)
    for d in range(1, ep):
        group = group + (first >= d * local).astype(jnp.int32)
    n_rows = info_out.shape[0]
    upper = (iota((tokens, tokens), 0) < iota((tokens, tokens), 1)).astype(F32).astype(BF16)
    g_rows = max(8, ep)
    member = (iota((g_rows, tokens), 0) == group).astype(F32)
    rank = jnp.sum(member * mm(member.astype(BF16), upper), 0, keepdims=True)
    slot = group.astype(F32) * cap + rank
    perm = (iota((tokens, tokens), 0).astype(F32) == slot).astype(F32)
    perm_s[...] = perm.astype(BF16)
    disp[...] = mm(perm.astype(BF16), x_ref[...]).astype(BF16)
    l0, l1 = ids[0:1] - group * local, ids[1:2] - group * local
    shares = share_ref[...]
    line = iota((n_rows, tokens), 0)
    picked = ((line == l0) | (line == l1)).astype(F32)
    shared = jnp.where(
        line - local == l0, shares[0:1], jnp.where(line - local == l1, shares[1:2], 0.0)
    )
    info = exact(jnp.where(line < local, picked, shared), perm, ROWS_ROWS)
    info_out[...] = info
    info_all[me] = info
    gall[mt] = gain_ref[...]
    sorted_rows = disp[...].astype(F32)
    sums = jnp.sum(sorted_rows * sorted_rows, -1, keepdims=True)
    sq_all[mt] = jnp.transpose(jnp.broadcast_to(sums, (tokens, tokens)))[:8]
    xall[mt, pl.ds(pl.multiple_of(me * cap, cap), cap), :] = disp[
        pl.ds(pl.multiple_of(me * cap, cap), cap), :
    ]

    def dispatch(step):
        to = nearest(step - 1)
        return remote(
            disp.at[pl.ds(pl.multiple_of(to * cap, cap), cap)],
            xall.at[mt, pl.ds(pl.multiple_of(me * cap, cap), cap)],
            d_send.at[to], d_recv.at[me], {"ep": to},
        )

    def tell(step):
        to = nearest(step - 1)
        return remote(info_out, info_all.at[me], i_send.at[to], i_recv.at[me], {"ep": to})

    def gains(step):
        to = lax.rem(mt + step, tp)
        return remote(gain_ref, gall.at[mt], g_send.at[to], g_recv.at[mt], {"tp": to})

    def squares(step):
        to = lax.rem(mt + step, tp)
        return remote(sq_all.at[mt], sq_all.at[mt], q_send.at[to], q_recv.at[mt], {"tp": to})

    def scales(step):
        to = nearest(step - 1)
        return remote(sc_out, sc_all.at[me], t_send.at[to], t_recv.at[me], {"ep": to})

    def send_scales():
        total = sq_all[mt]
        for step in range(1, tp):
            t = lax.rem(mt + step, tp)
            landed(sq_all.at[t], q_recv.at[t])
            total = total + sq_all[t]
        row = lax.rsqrt(total / (tp * dl) + EPSILON)
        sc_out[...] = row
        sc_all[me] = row
        for step in range(1, ep):
            scales(step).start()

    def chunk_of(origin, s):
        return xall.at[origin, pl.ds(pl.multiple_of(s * cap, cap), cap)]

    def over_x(step, s):
        to = lax.rem(chip + step, chips)
        part = chunk_of(mt, s)
        return remote(part, part, gx_send.at[to, s], gx_recv.at[chip, s], {"tp": to * 2 + core})

    def to_mate(step, s):
        origin = lax.rem(chip + step, chips)
        part = chunk_of(origin * 2 + core, s)
        return remote(part, part, gc_send.at[origin, s], gc_recv.at[origin, s], {"tp": mate})

    def expert_rows(e):
        return pl.ds(pl.multiple_of(e * cap_e, cap_e), cap_e)

    def h_over_x(step, e):
        to = lax.rem(chip + step, chips)
        return remote(
            hmine.at[expert_rows(e)], hall.at[mt, expert_rows(e)],
            hx_send.at[to, e], hx_recv.at[chip, e], {"tp": to * 2 + core},
        )

    def h_to_mate(step, e):
        origin = lax.rem(chip + step, chips)
        part = hall.at[origin * 2 + core, expert_rows(e)]
        src = hmine.at[expert_rows(e)] if step == 0 else part
        return remote(src, part, hc_send.at[origin, e], hc_recv.at[origin, e], {"tp": mate})

    def h_relay(e):
        for step in range(1, chips):
            origin = lax.rem(chip + step, chips)
            landed(hall.at[origin * 2 + core, expert_rows(e)], hx_recv.at[origin, e])
            h_to_mate(step, e).start()

    def giving(step, part):
        to = nearest(ep - 1 - step)
        lanes = slice(part * wide_part, (part + 1) * wide_part)
        return remote(
            ret_out.at[pl.ds(pl.multiple_of(to * cap, cap), cap), lanes],
            ret_in.at[pl.ds(pl.multiple_of(me * cap, cap), cap), lanes],
            r_send.at[to, part], r_recv.at[me, part], {"ep": to},
        )

    def landed(dst, sem):
        pltpu.make_async_copy(dst, dst, sem).wait()

    for copy in arriving[4:]:
        copy.wait()
    for which in range(3):
        for e in range(local):
            weight(which, e).start()

    pl.semaphore_wait(barrier, ep - 1 + tp - 1)
    for step in range(1, tp):
        squares(step).start()
    for step in range(1, ep):
        dispatch(step).start()
        tell(step).start()
    for step in range(1, tp):
        gains(step).start()

    def forward(j):
        s = nearest(j - 1) if j > 0 else me
        if j > 0:
            landed(chunk_of(mt, s), d_recv.at[s])
        for step in range(1, chips):
            over_x(step, s).start()
        to_mate(0, s).start()

    def relay(j):
        s = nearest(j - 1) if j > 0 else me
        for step in range(1, chips):
            origin = lax.rem(chip + step, chips)
            landed(chunk_of(origin * 2 + core, s), gx_recv.at[origin, s])
            to_mate(step, s).start()

    forward(0)

    for src, dst in ((k_ref, k_s), (v_ref, v_s), (q_ref, q_s)):
        flat_s[...] = src[...].astype(F32)
        for h in range(heads):
            for c in range(length // 128):
                dst[c * 128 : (c + 1) * 128, h * 128 : (h + 1) * 128] = flat_s[
                    pl.ds(c * 128 * heads + h, 128, stride=heads), :
                ].astype(BF16)

    strengths = 1.0 / (1.0 + jnp.exp(-beta_ref[...]))
    raw = decay_ref[...]
    small = jnp.exp(-jnp.abs(raw))
    bigger = 1.0 + small
    diff = bigger - 1.0
    log_term = jnp.where(
        diff == 0.0, small, jnp.log(bigger) * small / jnp.where(diff == 0.0, 1.0, diff)
    )
    rates = jnp.maximum(raw, 0.0) + log_term
    ones_upper = (iota((128, 128), 0) <= iota((128, 128), 1)).astype(F32)
    chunks = length // 128
    rows_s[...] = jnp.zeros_like(rows_s)
    for c in range(chunks):
        here = slice(c * 128, (c + 1) * 128)
        summed = -exact(rates[:, here], ones_upper)
        for h in range(heads):
            u = h * chunks + c
            rows_s[u : u + 1, :] = summed[h : h + 1]
            rows_s[heads * chunks + u : heads * chunks + u + 1, :] = strengths[h : h + 1, here]

    def chain_copy(h):
        return remote(sout_s.at[h], sin_s.at[h], c_send.at[h], c_recv.at[h], {"ep": lax.rem(me + 1, ep)})

    def carry_on():
        carry_all(k_s, v_s, rows_s, cols_s, inv_s, sc_s, qd_s, y_s, z_s, m_s, n_s)

        @pl.when(me == 0)
        def _():
            for h in range(heads):
                sout_s[h] = n_s[h].astype(BF16)
                chain_copy(h).start()

    def chain_turn(low, high):
        def turn(h, carry):
            landed(sin_s.at[h], c_recv.at[h])

            @pl.when(me < ep - 1)
            def _():
                sout_s[h] = (mm(m_s[h], twice(sin_s[h])) + n_s[h]).astype(BF16)
                chain_copy(h).start()

            return carry

        def all_turns():
            lax.fori_loop(low, high, turn, 0)

        return all_turns

    def outputs():
        outputs_all(heads, length // 128, sc_s, z_s, y_s)

    def early(place):
        if place == 1:
            send_scales()
            forward(1)
        elif place == 2:
            for j in range(2, ep):
                forward(j)
            relay(0)

    solve_all(q_s, k_s, rows_s, cols_s, qd_s, sc_s, inv_s, early)
    carry_on()

    for step in range(1, ep):
        s = lax.rem(me + step, ep)
        landed(info_all.at[s], i_recv.at[s])
    r_in, r_out = iota((ep * tokens, tokens), 0), iota((ep * tokens, tokens), 1)
    source = r_in // tokens
    takes = (r_in - source * tokens - me * cap == r_out - source * cap) & (r_out // cap == source)
    takes = takes.astype(F32).astype(BF16)
    left, told = joined([info_all[s] for s in range(ep)], 1), jnp.zeros((n_rows, tokens), F32)
    for piece in range(3):
        taken = left.astype(BF16)
        told = told + mm(taken, takes)
        left = left - taken.astype(F32)
    ranks = mm(told.astype(BF16), upper)
    for e in range(local):
        where_to = iota((cap_e, tokens), 0).astype(F32) == ranks[e : e + 1]
        placed = jnp.where(where_to, told[e : e + 1], 0.0)
        place_s[e * cap_e : (e + 1) * cap_e, :] = placed.astype(BF16)
        left = jnp.transpose(placed * told[local + e : local + e + 1])
        for piece in range(back_s.shape[0]):
            taken = left.astype(BF16)
            back_s[piece, :, e * cap_e : (e + 1) * cap_e] = taken
            left = left - taken.astype(F32)


    for j in range(1, ep):
        relay(j)
    for step in range(1, ep):
        s = lax.rem(me + step, ep)
        landed(sc_all.at[s], t_recv.at[s])
    left, row = joined([sc_all[s] for s in range(ep)], 1), jnp.zeros((8, tokens), F32)
    for piece in range(3):
        taken = left.astype(BF16)
        row = row + mm(taken, takes)
        left = left - taken.astype(F32)
    scale = jnp.transpose(jnp.broadcast_to(row[:1], (tokens, tokens)))[:, :1]
    for step in range(1, tp):
        t = lax.rem(mt + step, tp)
        landed(gall.at[t], g_recv.at[t])

    def origin_of(step):
        return lax.rem(chip + step, chips)

    def weights_of(step):
        return pl.ds(pl.multiple_of(origin_of(step) * 2 * dl, 2 * dl), 2 * dl)

    def gained(step):
        for side in range(2):
            t = origin_of(step) * 2 + side
            xw_s[:, side * dl : (side + 1) * dl] = (xall[t].astype(F32) * scale * gall[t]).astype(BF16)

    def mates(step):
        for s in range(ep):
            landed(chunk_of(origin_of(step) * 2 + 1 - core, s), gc_recv.at[origin_of(step), s])

    mates(0)
    gained(0)

    for e in range(local):
        weight(0, e).wait()
        weight(1, e).wait()
    for e in range(local):
        gacc_s[e] = mm(xw_s[...], wg_v[e, weights_of(0), :])
        uacc_s[e] = mm(xw_s[...], wu_v[e, weights_of(0), :])
    outputs()
    for step in range(1, chips - 1):
        mates(step)
        gained(step)
        for e in range(local):
            gacc_s[e] = gacc_s[e] + mm(xw_s[...], wg_v[e, weights_of(step), :])
            uacc_s[e] = uacc_s[e] + mm(xw_s[...], wu_v[e, weights_of(step), :])
    mates(chips - 1)
    gained(chips - 1)

    def sums(e):
        part = weights_of(chips - 1)
        return gacc_s[e] + mm(xw_s[...], wg_v[e, part, :]), uacc_s[e] + mm(xw_s[...], wu_v[e, part, :])

    following = sums(0)
    for e in range(local):
        rows = expert_rows(e)
        gate, up = following
        if e + 1 < local:
            following = sums(e + 1)
        hidden = (gate / (1.0 + jnp.exp(-gate)) * up).astype(BF16)
        hidden = mm(place_s[rows, :], hidden).astype(BF16)
        hmine[rows, :] = hidden
        hall[mt, rows, :] = hidden
        for step in range(1, chips):
            h_over_x(step, e).start()
        h_to_mate(0, e).start()

    pl.when(me == 1)(chain_turn(0, heads))

    def finals():
        for u in range(heads * chunks):
            h, c = u // chunks, u % chunks
            mixed = mm(sc_s[u], twice(sin_s[h])) + y_s[u]
            query = q_s[c * 128 : (c + 1) * 128, h * 128 : (h + 1) * 128].astype(F32)
            squared = jnp.sum(query * query, -1, keepdims=True) + EPSILON
            rq = lax.rsqrt(squared) * (128 ** (-0.5))
            factor = rq * lax.rsqrt(jnp.mean(mixed * mixed, -1, keepdims=True) * (rq * rq) + EPSILON)
            flat_s[pl.ds(c * 128 * heads + h, 128, stride=heads), :] = mixed * factor * ngain_ref[...]
        mix_ref[...] = flat_s[...].astype(BF16)

    @pl.when(me == 0)
    def _():
        sin_s[...] = jnp.zeros_like(sin_s)

    units = 2 * hall.shape[2]

    def hidden_of(step, e):
        rows = expert_rows(e)
        landed(hall.at[origin_of(step) * 2 + 1 - core, rows], hc_recv.at[origin_of(step), e])
        return joined([hall[origin_of(step) * 2 + side, rows, :] for side in range(2)], 1)

    def downs(step, e):
        return wd_v[e, pl.ds(pl.multiple_of(origin_of(step) * units, units), units), :]

    for e in range(local):
        weight(2, e).wait()
    for step in range(chips - 1):
        for e in range(local):
            rows = slice(e * cap_e, (e + 1) * cap_e)
            out = mm(hidden_of(step, e), downs(step, e))
            dacc_s[rows, :] = out if step == 0 else dacc_s[rows, :] + out
    for e in range(local):
        h_relay(e)
    pl.when(me == 2)(chain_turn(0, heads))
    for e in range(local):
        rows = slice(e * cap_e, (e + 1) * cap_e)
        out = dacc_s[rows, :] + mm(hidden_of(chips - 1, e), downs(chips - 1, e))
        copies_s[rows, :] = out.astype(BF16)
    own = pl.ds(pl.multiple_of(me * cap, cap), cap)
    for part in range(parts):
        lanes = slice(part * wide_part, (part + 1) * wide_part)
        result = mm(joined([back_s[piece] for piece in range(back_s.shape[0])], 1), twice(copies_s[:, lanes]))
        ret_out[:, lanes] = result.astype(BF16)
        ret_in[own, lanes] = ret_out[own, lanes]
        for step in range(1, ep):
            giving(step, part).start()

    pl.when(me >= 3)(chain_turn(0, heads))
    finals()
    for step in range(1, ep):
        s = lax.rem(me + step, ep)
        for part in range(parts):
            lanes = slice(part * wide_part, (part + 1) * wide_part)
            landed(ret_in.at[pl.ds(pl.multiple_of(s * cap, cap), cap), lanes], r_recv.at[s, part])
    ffn_ref[...] = mm(perm_s[...], ret_in[...], COLS_COLS).astype(BF16)

    for step in range(1, ep):
        dispatch(step).wait_send()
        scales(step).wait_send()
        tell(step).wait_send()
        for part in range(parts):
            giving(step, part).wait_send()
    for step in range(1, tp):
        gains(step).wait_send()
        squares(step).wait_send()
    for step in range(1, chips):
        for e in range(local):
            h_over_x(step, e).wait_send()
        for s in range(ep):
            over_x(step, s).wait_send()
    for step in range(chips):
        for e in range(local):
            h_to_mate(step, e).wait_send()
        for s in range(ep):
            to_mate(step, s).wait_send()

    @pl.when(me < ep - 1)
    def _():
        def sent(h, carry):
            chain_copy(h).wait_send()
            return carry

        lax.fori_loop(0, heads, sent, 0)


def hand_on(mix_ref, ffn_ref, mix_out, ffn_out, sems):
    copies = [
        pltpu.make_async_copy(mix_ref, mix_out, sems.at[0]),
        pltpu.make_async_copy(ffn_ref, ffn_out, sems.at[1]),
    ]
    for copy in copies:
        copy.start()
    for copy in copies:
        copy.wait()


def fused_body(
    mix_query, mix_keys, mix_values, beta_in, decay_in, norm_gain, ffn_input, ffn_gain,
    expert_ids, expert_share, w_gate, w_up, w_down,
):
    ep, tp = lax.axis_size("ep"), lax.axis_size("tp")
    length, heads, width = mix_query.shape
    tokens, dl = ffn_input.shape
    local, full, fl = w_gate.shape
    out_width = w_down.shape[2]
    picks = expert_ids.shape[1]
    n_rows = max(8, 2 * local)
    chips = tp // 2
    rows_e = tokens * picks
    parts = max(1, min(2, out_width // 512))
    dma = pltpu.SemaphoreType.DMA
    vmem = pl.BlockSpec(memory_space=pltpu.VMEM)
    units = heads * (length // width)
    mix_out, ffn_out = pl.pallas_call(
        layer_kernel,
        out_shape=(
            pltpu.VMEM((length * heads, width), BF16),
            pltpu.VMEM((tokens, out_width), BF16),
        ),
        in_specs=[pl.BlockSpec(memory_space=pltpu.HBM)] * 13,
        out_specs=(vmem, vmem),
        scratch_shapes=[
            pltpu.VMEM((length * heads, width), BF16),
            pltpu.VMEM((length * heads, width), BF16),
            pltpu.VMEM((length * heads, width), BF16),
            pltpu.VMEM(beta_in.shape, F32),
            pltpu.VMEM(decay_in.shape, F32),
            pltpu.VMEM((1, width), F32),
            pltpu.VMEM(ffn_input.shape, BF16),
            pltpu.VMEM((1, dl), F32),
            pltpu.VMEM((picks, tokens), jnp.int32),
            pltpu.VMEM((picks, tokens), F32),
            dma((10,)),
            pltpu.VMEM((length, heads * width), BF16),
            pltpu.VMEM((length, heads * width), BF16),
            pltpu.VMEM((length, heads * width), BF16),
            pltpu.VMEM((length * heads, width), F32),
            pltpu.VMEM((128, 128), F32),
            pltpu.VMEM((128, 128), F32),
            pltpu.VMEM((units, width, 2 * width), BF16),
            pltpu.VMEM((max(units - heads, 1), width, 2 * width), BF16),
            pltpu.VMEM((units, width, width), F32),
            pltpu.VMEM((units, width, width), F32),
            pltpu.VMEM((units, width, width), F32),
            pltpu.VMEM((heads, width, 2 * width), BF16),
            pltpu.VMEM((heads, width, width), F32),
            pltpu.VMEM((heads, width, width), BF16),
            pltpu.VMEM((heads, width, width), BF16),
            pltpu.VMEM(w_gate.shape, BF16),
            pltpu.VMEM(w_up.shape, BF16),
            pltpu.VMEM(w_down.shape, BF16),
            pltpu.VMEM((tokens, tokens), BF16),
            pltpu.VMEM((tokens, dl), BF16),
            pltpu.VMEM((n_rows, tokens), F32),
            pltpu.VMEM((ep, n_rows, tokens), F32),
            pltpu.VMEM((tp, 8, tokens), F32),
            pltpu.VMEM((8, tokens), F32),
            pltpu.VMEM((ep, 8, tokens), F32),
            pltpu.VMEM((tp, 1, dl), F32),
            pltpu.VMEM((tp, tokens, dl), BF16),
            pltpu.VMEM((tokens, full // chips), BF16),
            pltpu.VMEM((local, tokens, fl), F32),
            pltpu.VMEM((local, tokens, fl), F32),
            pltpu.VMEM((rows_e, fl), BF16),
            pltpu.VMEM((tp, rows_e, fl), BF16),
            pltpu.VMEM((rows_e, tokens), BF16),
            pltpu.VMEM((2, tokens, rows_e), BF16),
            pltpu.VMEM((rows_e, out_width), F32),
            pltpu.VMEM((rows_e, out_width), BF16),
            pltpu.VMEM((tokens, out_width), BF16),
            pltpu.VMEM((tokens, out_width), BF16),
            dma((3, local)),
            dma((ep,)), dma((ep,)), dma((ep,)), dma((ep,)),
            dma((tp,)), dma((tp,)), dma((tp,)), dma((tp,)),
            dma((ep,)), dma((ep,)),
            dma((chips, ep)), dma((chips, ep)), dma((chips, ep)), dma((chips, ep)),
            dma((chips, local)), dma((chips, local)), dma((chips, local)), dma((chips, local)),
            dma((ep, parts)), dma((ep, parts)),
            dma((heads,)), dma((heads,)),
        ],
        compiler_params=pltpu.CompilerParams(
            collective_id=0, has_side_effects=True, vmem_limit_bytes=60 * 1024 * 1024
        ),
    )(
        mix_query.reshape(length * heads, width),
        mix_keys.reshape(length * heads, width),
        mix_values.reshape(length * heads, width),
        beta_in, decay_in, norm_gain.reshape(1, width),
        ffn_input, ffn_gain.reshape(1, dl), expert_ids.T, expert_share.T,
        w_gate, w_up, w_down,
    )
    mix_out, ffn_out = pl.pallas_call(
        hand_on,
        out_shape=(
            jax.ShapeDtypeStruct(mix_out.shape, BF16),
            jax.ShapeDtypeStruct(ffn_out.shape, BF16),
        ),
        in_specs=[vmem] * 2,
        out_specs=(pl.BlockSpec(memory_space=pltpu.HBM),) * 2,
        scratch_shapes=[dma((2,))],
        cost_estimate=pl.CostEstimate(flops=1000, bytes_accessed=2**21, transcendentals=0),
        compiler_params=pltpu.CompilerParams(vmem_limit_bytes=4 * 1024 * 1024),
    )(mix_out, ffn_out)
    return (mix_out.reshape(length, heads, width), ffn_out)


def body(
    mix_query,
    mix_keys,
    mix_values,
    beta_in,
    decay_in,
    norm_gain,
    ffn_input,
    ffn_gain,
    expert_ids,
    expert_share,
    w_gate,
    w_up,
    w_down,
):
    width, local = mix_query.shape[2], w_gate.shape[0]
    whole_groups = local % GROUP == 0 and expert_ids.shape[1] == 2
    even = lax.axis_size("tp") % 2 == 0 and lax.axis_size("tp") > 1 and lax.axis_size("ep") > 1
    units = mix_query.shape[1] * mix_query.shape[0] // 128
    if whole_groups and even and units % 8 == 0 and units < 25 and width == 128 and mix_query.shape[0] % 128 == 0:
        return fused_body(
            mix_query,
            mix_keys,
            mix_values,
            beta_in,
            decay_in,
            norm_gain,
            ffn_input,
            ffn_gain,
            expert_ids,
            expert_share,
            w_gate,
            w_up,
            w_down,
        )
    mix_out = mixer_body(mix_query, mix_keys, mix_values, beta_in, decay_in, norm_gain)
    ffn_out = experts_body(ffn_input, ffn_gain, expert_ids, expert_share, w_gate, w_up, w_down)
    return (mix_out, ffn_out)


def solution(mesh):
    placed = (
        P(("grp", "ep"), "tp", None),
        P(("grp", "ep"), "tp", None),
        P(("grp", "ep"), "tp", None),
        P("tp", ("grp", "ep")),
        P("tp", ("grp", "ep")),
        P(),
        P(("grp", "ep"), "tp"),
        P("tp"),
        P(("grp", "ep"), None),
        P(("grp", "ep"), None),
        P("ep", None, "tp"),
        P("ep", None, "tp"),
        P("ep", None, "tp"),
    )
    return jax.shard_map(
        body,
        mesh=mesh,
        in_specs=placed,
        out_specs=(P(("grp", "ep"), "tp", None), P(("grp", "ep"), "tp")),
        check_vma=False,
    )
```
